32 devices in a mesh: ep: 8 (over z, x), tp: 4 (over y, core).
Axes of the slice: x: 2, y: 2, z: 4, core: 2. Of those that a mesh axis runs over, the one named last changes fastest.
Arguments:
- tokens: bfloat16 [32, 2048], P(('ep', 'tp')), may hold values from -6 to 6
- norm_gain: float32 [2048], replicated, may hold values from 0.1 to 1.9
- w_query: bfloat16 [2048, 4096], P('ep', 'tp'), may hold values from -0.125 to 0.125
- w_key: bfloat16 [2048, 512], P('ep', 'tp'), may hold values from -0.125 to 0.125
- w_value: bfloat16 [2048, 512], P('ep', 'tp'), may hold values from -0.125 to 0.125
- key_cache: bfloat16 [32, 1024, 512], P(('ep', 'tp')), may hold values from -900 to 900
- value_cache: bfloat16 [32, 1024, 512], P(('ep', 'tp')), may hold values from -6 to 6
- lengths: int32 [32], P(('ep', 'tp')), may hold values from 512 to 1023, as said below
- diff_lambda: float32 [16], replicated, may hold values from 0.3 to 0.8
- head_gain: float32 [256], replicated, may hold values from 0.1 to 1.9
- w_out: bfloat16 [4096, 2048], P('tp', 'ep'), may hold values from -0.09375 to 0.09375
- ffn_gain: float32 [2048], replicated, may hold values from 0.1 to 1.9
- routing: int32 [32, 2], P('ep'), may hold values from 0 to 7, all different within a row; in each aligned block of 4 rows (0 to 3, 4 to 7, ...) at most 4 rows name the same one
- route_weight: float32 [32, 2], P('ep'), may hold values from 0.2 to 1
- w_gate: bfloat16 [8, 2048, 3584], P('ep', None, 'tp'), may hold values from -0.125 to 0.125
- w_up: bfloat16 [8, 2048, 3584], P('ep', None, 'tp'), may hold values from -0.125 to 0.125
- w_down: bfloat16 [8, 3584, 2048], P('ep', 'tp'), may hold values from -0.09375 to 0.09375
Outputs:
- result: bfloat16 [32, 2048], P(('ep', 'tp'))
- new_keys: bfloat16 [32, 512], P(('ep', 'tp'))
- new_values: bfloat16 [32, 512], P(('ep', 'tp'))
The draws below stay inside these ranges and needn't reach their ends.
Inputs may be any that keep to these rules, and one draw needn't show every extreme that they name: Each sequence's new token sits at position lengths[s], just after its valid cached positions. `routing`: each row names 2 different experts. In each aligned block of 4 rows (one ep index's sequences) no expert is named by more than 4 rows.
All inputs are finite; a program needn't handle non-finite values.
Results may differ from the reference program's by a relative error of at most 0.017.
Values may be sent and summed in bfloat16 or wider, within the bound.
A program may use at most 64 MiB of HBM per device.

```python
import math
import jax
import jax.numpy as jnp
import numpy as np
from jax import lax

D = 2048
HEADS = 16
KV_HEADS = 2
HEAD_QK = 128
HEAD_V = 256
FE = 3584
TOPK = 2
LEN = 1024
GROUP = 4
SEQS = 32
EXPERTS = 8
CAP = 4
N_EP = 8
N_TP = 4


def draw_key_cache(key, part):
    base = jax.random.normal(key, (SEQS, LEN, KV_HEADS * 2 * HEAD_QK), jnp.float32)
    base = jnp.clip(base, -8.0, 8.0) * 1.75
    return base.astype(jnp.bfloat16)


def draw_lengths(key, part):
    drawn = jax.random.randint(key, (SEQS,), LEN // 2, LEN)
    longest = jax.random.randint(jax.random.fold_in(key, 3), (), 0, SEQS)
    return jnp.where(jnp.arange(SEQS) == longest, LEN - 1, drawn).astype(jnp.int32)


def shard_levels(stream_key, shape, pieces, smallest, top_value):
    loudness = 1.0
    for axis_at, shards_of in pieces:
        heights = jax.random.uniform(jax.random.fold_in(jax.random.fold_in(stream_key, 6), axis_at), (shards_of,), jnp.float32, smallest / len(pieces), top_value / len(pieces))
        loudness = loudness * jnp.repeat(jnp.exp(heights), shape[axis_at] // shards_of).reshape((-1,) + (1,) * (len(shape) - 1 - axis_at))
    return loudness


def shared_out(own_key, own, number, rows, number_of, top, reach, skew):
    ranking = jax.random.permutation(own_key, number_of)
    packed, ordinary = portions_of(number_of, rows * top, reach, skew, True), portions_of(number_of, rows * top, reach, skew, False)
    places = jnp.arange(number_of)

    def named(tallies, offset_by):
        used = int((tallies > 0).sum())
        fixed = max(1, used // 4)
        passed = fixed + (places - fixed + offset_by * (used - fixed)) % max(1, number_of - fixed)
        return jnp.zeros((number_of,), jnp.int32).at[ranking[jnp.where(places < fixed, places, passed)]].set(jnp.asarray(tallies, jnp.int32))

    tallies = jnp.where(number % 4 == 0, named(packed, number // 4), named(ordinary, number - number // 4 - 1))
    mixed = jax.random.permutation(jax.random.fold_in(own, 3), number_of)
    giver, sink = mixed[0:number_of // 2 * 2:2], mixed[1:number_of // 2 * 2:2]
    room = jnp.minimum(tallies[giver] - 1, reach - tallies[sink]) // 2
    room = jnp.where((giver == ranking[0]) | (sink == ranking[0]) | (tallies[sink] == 0), 0, jnp.maximum(room, 0))
    passed = jax.random.randint(jax.random.fold_in(own, 4), (number_of // 2,), 0, 1 << 20) % (room + 1)
    tallies = tallies.at[giver].add(-passed).at[sink].add(passed)
    labels = jnp.searchsorted(jnp.cumsum(tallies), jnp.arange(rows * top), side="right").astype(jnp.int32)
    grid = labels.reshape(top, rows).T
    grid = grid[jax.random.permutation(jax.random.fold_in(own, 1), rows)]
    offset_by = jax.random.randint(jax.random.fold_in(own, 2), (rows, 1), 0, top)
    return jnp.take_along_axis(grid, (jnp.arange(top)[None, :] + offset_by) % top, axis=1)


def portions_of(number_of, total, limit, slope, full):
    loads = [(1 << 20) // math.isqrt(grade ** slope) + 1 for grade in range(1, number_of + 1)]
    largest = limit if full else min(limit, max(-(-total // number_of), total * loads[0] // sum(loads)))
    least = 1 if total - largest >= number_of - 1 else 0
    given, rest = [largest] + [least] * (number_of - 1), total - largest - least * (number_of - 1)
    while rest > 0:
        free = [i for i in range(1, number_of) if given[i] < largest] or [i for i in range(1, number_of) if given[i] < limit]
        mass, budget = sum([loads[i] for i in free]), rest
        for i in free:
            extra = min(limit - given[i], max(1, budget * loads[i] // mass), rest)
            given[i] = given[i] + extra
            rest = rest - extra
    return np.array(given)


def normal_values(rng, shape, width, limit, split=(), kind=jnp.bfloat16):
    array = jax.random.normal(rng, shape, jnp.float32) * width
    if len(split) > 0:
        array = shard_levels(rng, shape, split, -0.22, 0.18) * array
    return jnp.clip(array, min=-limit, max=limit).astype(kind)


def setup_inputs(seed: int = 0) -> dict:
    key_of = jax.random.split(jax.random.key(seed), 18)
    tokens = normal_values(key_of[0], (SEQS, D), 1.0, 6.0, ((0, 32),))
    norm_gain = jnp.clip(1.0 + 0.18 * jax.random.normal(key_of[1], (D,), jnp.float32), 0.1, 1.9)
    w_query = normal_values(key_of[2], (D, HEADS * 2 * HEAD_QK), D ** -0.5, 0.125, ((0, 8), (1, 4)))
    w_key = normal_values(key_of[3], (D, KV_HEADS * 2 * HEAD_QK), D ** -0.5, 0.125, ((0, 8), (1, 4)))
    w_value = normal_values(key_of[4], (D, KV_HEADS * HEAD_V), D ** -0.5, 0.125, ((0, 8), (1, 4)))
    key_cache = draw_key_cache(jax.random.fold_in(key_of[17], 71), 0)
    value_cache = normal_values(key_of[6], (SEQS, LEN, KV_HEADS * HEAD_V), 1.0, 6.0, ((0, 32),))
    lengths = draw_lengths(jax.random.fold_in(key_of[17], 71), 0)
    diff_lambda = jnp.clip(jax.random.uniform(key_of[8], (HEADS,), jnp.float32, 0.3, 0.8), 0.3, 0.8)
    head_gain = jnp.clip(1.0 + 0.18 * jax.random.normal(key_of[9], (HEAD_V,), jnp.float32), 0.1, 1.9)
    w_out = normal_values(key_of[10], (HEADS * HEAD_V, D), (HEADS * HEAD_V) ** -0.5, 0.09375, ((0, 4), (1, 8)))
    ffn_gain = jnp.clip(1.0 + 0.18 * jax.random.normal(key_of[11], (D,), jnp.float32), 0.1, 1.9)
    routing_keys = jax.random.split(jax.random.fold_in(key_of[12], 1), SEQS // GROUP)
    routing_turns = jax.random.permutation(jax.random.fold_in(key_of[12], 3), SEQS // GROUP)
    routing = jax.vmap(lambda own, number: shared_out(jax.random.fold_in(key_of[12], 2), own, number, GROUP, EXPERTS, TOPK, CAP, 2))(routing_keys, routing_turns).reshape((SEQS, TOPK))
    route_weight = jnp.clip(0.2 + 0.8 * jax.random.uniform(key_of[13], (SEQS, TOPK), jnp.float32) ** shard_levels(key_of[13], (SEQS, TOPK), ((0, 8),), -0.2, 0.2), 0.2, 1.0)
    w_gate = normal_values(key_of[14], (EXPERTS, D, FE), D ** -0.5, 0.125, ((0, 8), (2, 4)))
    w_up = normal_values(key_of[15], (EXPERTS, D, FE), D ** -0.5, 0.125, ((0, 8), (2, 4)))
    w_down = normal_values(key_of[16], (EXPERTS, FE, D), FE ** -0.5, 0.09375, ((0, 8), (1, 4)))
    return {"tokens": tokens, "norm_gain": norm_gain, "w_query": w_query, "w_key": w_key, "w_value": w_value, "key_cache": key_cache, "value_cache": value_cache, "lengths": lengths, "diff_lambda": diff_lambda, "head_gain": head_gain, "w_out": w_out, "ffn_gain": ffn_gain, "routing": routing, "route_weight": route_weight, "w_gate": w_gate, "w_up": w_up, "w_down": w_down}


NORM_EPS = 1e-05
HEAD_EPS = 0.01
HEAD_SCALE = 0.8

def rms_scale(values, gain_row, floor_add):
    mean_sq = lax.optimization_barrier(jnp.mean(values * values, axis=-1, keepdims=True))
    return values * lax.rsqrt(mean_sq + floor_add) * gain_row

def attend_one(inputs, diff_lambda, head_gain):
    queries, key_row, value_row, cache_keys, cache_vals, length = inputs
    repeat = HEADS // KV_HEADS
    queries = queries.reshape(KV_HEADS, repeat, 2, HEAD_QK).astype(jnp.float32)
    key_row = key_row.reshape(KV_HEADS, 2, HEAD_QK).astype(jnp.float32)
    value_row = value_row.reshape(KV_HEADS, HEAD_V).astype(jnp.float32)
    cache_keys = cache_keys.reshape(LEN, KV_HEADS, 2, HEAD_QK).astype(jnp.float32)
    cache_vals = cache_vals.reshape(LEN, KV_HEADS, HEAD_V).astype(jnp.float32)
    score_scale = HEAD_QK ** (-0.5)
    cached = jnp.einsum('grcd,lgcd->grcl', queries, cache_keys) * score_scale
    own_score = jnp.einsum('grcd,gcd->grc', queries, key_row) * score_scale
    in_range = jnp.arange(LEN) < length
    cached = jnp.where(in_range, cached, -jnp.inf)
    row_peak = jnp.maximum(lax.optimization_barrier(jnp.max(cached, axis=-1)), own_score)
    cached_w = jnp.exp(cached - row_peak[..., None])
    own_w = jnp.exp(own_score - row_peak)
    row_total = lax.optimization_barrier(jnp.sum(cached_w, axis=-1)) + own_w
    cached_w = cached_w / row_total[..., None]
    own_w = own_w / row_total
    lam_heads = diff_lambda.reshape(KV_HEADS, repeat)
    mix_cached = (cached_w[:, :, 0] - lam_heads[..., None] * cached_w[:, :, 1]).astype(jnp.bfloat16)
    mix_own = (own_w[..., 0] - lam_heads * own_w[..., 1]).astype(jnp.bfloat16)
    head_raw = jnp.einsum('grl,lgv->grv', mix_cached.astype(jnp.float32), cache_vals)
    head_raw = head_raw + mix_own.astype(jnp.float32)[..., None] * value_row[:, None, :]
    head_out = rms_scale(head_raw, head_gain, HEAD_EPS) * HEAD_SCALE
    return head_out.astype(jnp.bfloat16).reshape(HEADS * HEAD_V)

def expert_apply(rows_in, gate_w, up_w, down_w):
    gate_pre = jnp.dot(rows_in, gate_w, preferred_element_type=jnp.float32)
    up_pre = jnp.dot(rows_in, up_w, preferred_element_type=jnp.float32)
    hidden = (jax.nn.silu(gate_pre) * up_pre).astype(jnp.bfloat16)
    span = FE // N_TP
    hidden_grp = hidden.reshape(-1, N_TP, span).astype(jnp.float32)
    down_grp = down_w.reshape(N_TP, span, D).astype(jnp.float32)
    partial_value = jnp.einsum('rgk,gkd->grd', hidden_grp, down_grp)
    partial_value = lax.optimization_barrier(partial_value.astype(jnp.bfloat16))
    return lax.optimization_barrier(jnp.sum(partial_value.astype(jnp.float32), axis=0)).astype(jnp.bfloat16)

def reference(tokens, norm_gain, w_query, w_key, w_value, key_cache, value_cache, lengths, diff_lambda, head_gain, w_out, ffn_gain, routing, route_weight, w_gate, w_up, w_down):
    normed = rms_scale(tokens.astype(jnp.float32), norm_gain, NORM_EPS).astype(jnp.bfloat16)
    queries = jnp.dot(normed, w_query, preferred_element_type=jnp.float32).astype(jnp.bfloat16)
    new_keys = jnp.dot(normed, w_key, preferred_element_type=jnp.float32).astype(jnp.bfloat16)
    new_values = jnp.dot(normed, w_value, preferred_element_type=jnp.float32).astype(jnp.bfloat16)
    head_all = lax.map(lambda item: attend_one(item, diff_lambda, head_gain), (queries, new_keys, new_values, key_cache, value_cache, lengths))
    attn_sum = jnp.dot(head_all, w_out, preferred_element_type=jnp.float32)
    residual = tokens.astype(jnp.float32) + attn_sum
    ffn_in = rms_scale(residual, ffn_gain, NORM_EPS).astype(jnp.bfloat16)
    picks = routing.reshape(N_EP, GROUP * TOPK).astype(jnp.int32)
    choose = (picks[:, :, None] == jnp.arange(N_EP, dtype=jnp.int32)[None, None, :]).astype(jnp.int32)
    earlier = jnp.cumsum(choose, axis=1) - choose
    slot_in = lax.optimization_barrier(jnp.sum(earlier * choose, axis=2)).astype(jnp.int32)
    group_idx = jnp.broadcast_to(jnp.arange(N_EP, dtype=jnp.int32)[:, None], picks.shape)
    token_ids = (group_idx * GROUP + jnp.arange(GROUP * TOPK, dtype=jnp.int32)[None, :] // TOPK).astype(jnp.int32)
    table = jnp.zeros((N_EP, N_EP, CAP), jnp.int32)
    table = table.at[picks, group_idx, slot_in].set(token_ids)

    def one_expert(item):
        index_rows, gate_w, up_w, down_w = item
        return expert_apply(ffn_in[index_rows.reshape(-1)], gate_w, up_w, down_w)
    outputs = lax.map(one_expert, (table, w_gate, w_up, w_down))
    outputs = outputs.reshape(N_EP, N_EP, CAP, D)
    picked = outputs[picks, group_idx, slot_in].reshape(SEQS, TOPK, D).astype(jnp.float32)
    ffn_out = lax.optimization_barrier(jnp.sum(picked * route_weight[:, :, None], axis=1))
    return ((residual + ffn_out).astype(jnp.bfloat16), new_keys, new_values)
```

```python
import functools

import jax
import jax.numpy as jnp
from jax import lax
from jax.experimental import pallas as pl
from jax.experimental.pallas import tpu as pltpu
from jax.sharding import PartitionSpec as P

HEADS = 16
KV_HEADS = 2
HEAD_QK = 128
HEAD_V = 256
TOPK = 2
LEN = 1024
SEQ_DEV = 1


NORM_EPS = 1e-05
HEAD_EPS = 0.01
HEAD_SCALE = 0.8


def rms_scale(values, gain_row, floor_add):
    mean_sq = jnp.mean(values * values, axis=-1, keepdims=True)
    return values * lax.rsqrt(mean_sq + floor_add) * gain_row


def attend(queries, key_rows, value_rows, key_cache, value_cache, lengths, diff_lambda, head_gain):
    row_count = queries.shape[0]
    repeat = HEADS // KV_HEADS
    queries = queries.reshape(row_count, KV_HEADS, repeat, 2, HEAD_QK)
    key_rows = key_rows.reshape(row_count, KV_HEADS, 2, HEAD_QK)
    value_rows = value_rows.reshape(row_count, KV_HEADS, HEAD_V)
    cache_keys = key_cache.reshape(row_count, LEN, KV_HEADS, 2, HEAD_QK)
    cache_vals = value_cache.reshape(row_count, LEN, KV_HEADS, HEAD_V)
    score_scale = HEAD_QK ** (-0.5)
    cached = (
        jnp.einsum("sgrcd,slgcd->sgrcl", queries, cache_keys, preferred_element_type=jnp.float32)
        * score_scale
    )
    own_score = (
        jnp.einsum("sgrcd,sgcd->sgrc", queries, key_rows, preferred_element_type=jnp.float32)
        * score_scale
    )
    in_range = jnp.arange(LEN)[None, :] < lengths[:, None]
    cached = jnp.where(in_range[:, None, None, None, :], cached, -jnp.inf)
    row_peak = jnp.maximum(jnp.max(cached, axis=-1), own_score)
    cached_w = jnp.exp(cached - row_peak[..., None])
    own_w = jnp.exp(own_score - row_peak)
    row_total = jnp.sum(cached_w, axis=-1) + own_w
    cached_w = cached_w / row_total[..., None]
    own_w = own_w / row_total
    lam_heads = diff_lambda.reshape(1, KV_HEADS, repeat)
    mix_cached = (cached_w[:, :, :, 0] - lam_heads[..., None] * cached_w[:, :, :, 1]).astype(
        jnp.bfloat16
    )
    mix_own = (own_w[..., 0] - lam_heads * own_w[..., 1]).astype(jnp.bfloat16)
    head_raw = jnp.einsum(
        "sgrl,slgv->sgrv", mix_cached, cache_vals, preferred_element_type=jnp.float32
    )
    head_raw = (
        head_raw
        + mix_own.astype(jnp.float32)[..., None] * value_rows.astype(jnp.float32)[:, :, None, :]
    )
    head_out = rms_scale(head_raw, head_gain, HEAD_EPS) * HEAD_SCALE
    return head_out.astype(jnp.bfloat16).reshape(row_count, HEADS * HEAD_V)


def body(
    tokens,
    norm_gain,
    w_query,
    w_key,
    w_value,
    key_cache,
    value_cache,
    lengths,
    diff_lambda,
    head_gain,
    w_out,
    ffn_gain,
    routing,
    route_weight,
    w_gate,
    w_up,
    w_down,
):
    group_tokens = lax.all_gather(tokens, "tp", axis=0, tiled=True)
    normed = rms_scale(group_tokens.astype(jnp.float32), norm_gain, NORM_EPS).astype(jnp.bfloat16)
    blocks = lax.all_to_all(normed, "ep", split_axis=1, concat_axis=0, tiled=True)
    query_term = jnp.dot(blocks, w_query, preferred_element_type=jnp.float32)
    key_term = jnp.dot(blocks, w_key, preferred_element_type=jnp.float32)
    value_term = jnp.dot(blocks, w_value, preferred_element_type=jnp.float32)
    query_sum, key_sum, value_sum = (
        lax.psum_scatter(query_term, "ep", scatter_dimension=0, tiled=True),
        lax.psum_scatter(key_term, "ep", scatter_dimension=0, tiled=True),
        lax.psum_scatter(value_term, "ep", scatter_dimension=0, tiled=True),
    )
    queries = query_sum.astype(jnp.bfloat16)
    keys_made = key_sum.astype(jnp.bfloat16)
    values_made = value_sum.astype(jnp.bfloat16)
    own_query, new_keys, new_values = (
        lax.all_to_all(queries, "tp", split_axis=0, concat_axis=1, tiled=True),
        lax.all_to_all(keys_made, "tp", split_axis=0, concat_axis=1, tiled=True),
        lax.all_to_all(values_made, "tp", split_axis=0, concat_axis=1, tiled=True),
    )
    head_out = attend(
        own_query, new_keys, new_values, key_cache, value_cache, lengths, diff_lambda, head_gain
    )
    head_rows = lax.all_to_all(head_out, "tp", split_axis=1, concat_axis=0, tiled=True)
    partial_out = jnp.dot(
        head_rows,
        lax.all_gather(w_out, "ep", axis=1, tiled=True),
        preferred_element_type=jnp.float32,
    )
    attn_sum = lax.psum_scatter(
        partial_out.astype(jnp.bfloat16), "tp", scatter_dimension=0, tiled=True
    ).astype(jnp.float32)
    residual = tokens.astype(jnp.float32) + attn_sum
    ffn_in = rms_scale(residual, ffn_gain, NORM_EPS).astype(jnp.bfloat16)
    group_in = lax.all_gather(ffn_in, "tp", axis=0, tiled=True)
    experts = lax.axis_size("ep")
    capacity = 8 * SEQ_DEV * lax.axis_size("tp") // experts
    group_rows = group_in.shape[0]
    picks = routing.reshape(-1)
    choose = (picks[:, None] == jnp.arange(experts)[None, :]).astype(jnp.int32)
    earlier = jnp.cumsum(choose, axis=0) - choose
    slot_in = jnp.sum(earlier * choose, axis=1)
    slot_ids = (picks * capacity + slot_in).reshape(group_rows, TOPK)
    slot_hit = slot_ids[:, :, None] == jnp.arange(experts * capacity)[None, None, :]
    dispatch = jnp.sum(slot_hit, axis=1).astype(jnp.bfloat16)
    outgoing = jnp.einsum(
        "rj,rd->jd", dispatch, group_in, preferred_element_type=jnp.float32
    ).astype(jnp.bfloat16)
    outgoing = outgoing.reshape(experts, capacity, group_in.shape[1])
    arrived = lax.all_to_all(outgoing, "ep", split_axis=0, concat_axis=0, tiled=True)
    sources, slot_count, feat_dim = arrived.shape
    flat_rows = arrived.reshape(sources * slot_count, feat_dim)
    gate_pre = jnp.dot(flat_rows, w_gate[0], preferred_element_type=jnp.float32)
    up_pre = jnp.dot(flat_rows, w_up[0], preferred_element_type=jnp.float32)
    hidden = (jax.nn.silu(gate_pre) * up_pre).astype(jnp.bfloat16)
    partial_down = jnp.dot(hidden, w_down[0], preferred_element_type=jnp.float32)
    summed = lax.psum_scatter(
        partial_down.astype(jnp.bfloat16), "tp", scatter_dimension=1, tiled=True
    )
    expert_rows = summed.reshape(sources, slot_count, summed.shape[1])
    returned = lax.all_to_all(expert_rows, "ep", split_axis=0, concat_axis=0, tiled=True)
    combine = jnp.sum(slot_hit.astype(jnp.float32) * route_weight[:, :, None], axis=1)
    flat_back = returned.reshape(experts * capacity, returned.shape[2]).astype(jnp.float32)
    moe_cols = jnp.dot(combine, flat_back, precision=lax.Precision.HIGHEST)
    moe_own = lax.all_to_all(moe_cols, "tp", split_axis=0, concat_axis=1, tiled=True)
    return ((residual + moe_own).astype(jnp.bfloat16), new_keys, new_values)


F32 = jnp.float32
BF16 = jnp.bfloat16
LANES = 128


def fused_kernel(
    ep_size,
    tp_size,
    tok_hbm,
    norm_gain_hbm,
    wq_hbm,
    wk_hbm,
    wv_hbm,
    kc_hbm,
    vc_hbm,
    len_s,
    lam_hbm,
    head_gain_hbm,
    wo_hbm,
    ffn_gain_hbm,
    routing_hbm,
    rweight_hbm,
    wg_hbm,
    wu_hbm,
    wd_hbm,
    out_ref,
    nk_ref,
    nv_ref,
    tok_v,
    norm_gain,
    head_gain,
    ffn_gain,
    lam_s,
    routing_s,
    rweight_s,
    wqkv,
    kc,
    vc,
    wo,
    wg,
    wu,
    wd,
    a_send,
    a_recv,
    b_send,
    b_recv,
    c_send,
    c_recv,
    r_send,
    r_recv,
    e_send,
    e_recv,
    stage,
    raw_keep,
    gate_acc,
    up_acc,
    load_sems,
    send_sems,
    recv_sems,
    block_sems,
    wo_send_sems,
    wo_recv_sems,
):
    n_dev = ep_size * tp_size
    my_ep = lax.axis_index("ep")
    my_tp = lax.axis_index("tp")
    me = my_ep * tp_size + my_tp
    width = tok_v.shape[1]
    feat = width // ep_size
    pieces = feat // LANES
    q_cols = wq_hbm.shape[1]
    q_rows = q_cols // LANES
    repeat = HEADS // KV_HEADS
    tile_rows = width // LANES
    seq_ep = ep_size

    def flips(index, size):
        bits = [lax.rem(index // (1 << b), 2) for b in range(size.bit_length() - 1)]
        return [
            sum(
                ((1 - bit) if (mask >> b) & 1 else bit) * (1 << b)
                for b, bit in enumerate(bits)
            )
            for mask in range(size)
        ]

    ep_of = flips(my_ep, ep_size)
    tp_of = flips(my_tp, tp_size)
    everyone = [
        (i, j) for i in reversed(range(ep_size)) for j in reversed(range(tp_size)) if i or j
    ]
    ep_peers = [(i, 0) for i in reversed(range(1, ep_size))]

    barrier = pltpu.get_barrier_semaphore()
    for i, j in everyone:
        pl.semaphore_signal(
            barrier,
            inc=1,
            device_id={"ep": ep_of[i], "tp": tp_of[j]},
            device_id_type=pl.DeviceIdType.MESH,
        )

    rows_half = wo_hbm.shape[0] // 2
    load_list = [
        (tok_hbm, tok_v),
        (norm_gain_hbm, norm_gain),
        (wq_hbm, wqkv.at[:, pl.ds(0, q_cols)]),
        (wk_hbm, wqkv.at[:, pl.ds(q_cols, LANES)]),
        (wv_hbm, wqkv.at[:, pl.ds(q_cols + LANES, LANES)]),
        (kc_hbm.at[0], kc),
        (vc_hbm.at[0], vc),
        (lam_hbm, lam_s),
        (head_gain_hbm, head_gain),
        (wo_hbm, wo.at[my_tp]),
        (ffn_gain_hbm, ffn_gain),
        (routing_hbm, routing_s),
        (rweight_hbm, rweight_s),
        (wg_hbm.at[0], wg),
        (wu_hbm.at[0], wu),
        (wd_hbm.at[0], wd),
    ]
    loads = [
        pltpu.make_async_copy(src, dst, load_sems.at[i]) for i, (src, dst) in enumerate(load_list)
    ]
    for load in loads:
        load.start()

    def ship(src, dst, i, j, send_sem, recv_sem):
        copy = pltpu.make_async_remote_copy(
            src_ref=src,
            dst_ref=dst,
            send_sem=send_sem,
            recv_sem=recv_sem,
            device_id={"ep": ep_of[i], "tp": tp_of[j]},
            device_id_type=pl.DeviceIdType.MESH,
        )
        copy.start()
        return copy

    def arrive(target, sem):
        pltpu.make_async_copy(target, target, sem).wait()

    loads[0].wait()
    loads[1].wait()
    tok = tok_v[...].astype(F32)
    mean_sq = jnp.mean(tok * tok, axis=-1, keepdims=True)
    normed = tok * lax.rsqrt(mean_sq + NORM_EPS) * norm_gain[...]
    for e in range(ep_size):
        for p in range(pieces):
            cols = slice(e * feat + p * LANES, e * feat + (p + 1) * LANES)
            stage[e * 8 + p : e * 8 + p + 1, :] = normed[:, cols]
            stage[e * 8 + pieces + p : e * 8 + pieces + p + 1, :] = tok[:, cols]
    a_send[...] = stage[0 : ep_size * 8, :].astype(BF16).reshape(ep_size, 8, LANES)
    a_recv[me] = a_send[my_ep]
    pl.semaphore_wait(barrier, n_dev - 1)
    for i, j in everyone:
        ship(a_send.at[ep_of[i]], a_recv.at[me], i, j, send_sems.at[0], recv_sems.at[0])
    wo_ships = [
        ship(
            wo_hbm.at[pl.ds(0, rows_half)],
            wo.at[my_tp, pl.ds(0, rows_half)],
            0,
            2,
            wo_send_sems.at[0],
            wo_recv_sems.at[0],
        )
    ]
    arrive(a_recv.at[pl.ds(0, n_dev - 1)], recv_sems.at[0])
    stage[0 : n_dev * 8, :] = a_recv[...].astype(F32).reshape(n_dev * 8, LANES)
    blocks = jnp.concatenate(
        [stage[pl.ds(p, n_dev, stride=8), :] for p in range(pieces)], axis=1
    ).astype(BF16)
    for p in range(pieces):
        raw_keep[:, p * LANES : (p + 1) * LANES] = stage[
            pl.ds(my_tp * 8 + pieces + p, ep_size, stride=8 * tp_size), :
        ]

    for i in range(2, 5):
        loads[i].wait()
    proj = jnp.dot(blocks, wqkv[...], preferred_element_type=F32)
    for j in range(q_rows + 2):
        stage[pl.ds(j, n_dev, stride=16), :] = proj[:, j * LANES : (j + 1) * LANES]
    b_send[...] = stage[...].astype(BF16).reshape(n_dev, 16, LANES)
    for i, j in everyone:
        to = ep_of[i] * tp_size + tp_of[j]
        ship(b_send.at[to], b_recv.at[me], i, j, send_sems.at[1], recv_sems.at[1])
    wo_ships.append(
        ship(
            wo_hbm.at[pl.ds(rows_half, rows_half)],
            wo.at[my_tp, pl.ds(rows_half, rows_half)],
            0,
            2,
            wo_send_sems.at[1],
            wo_recv_sems.at[1],
        )
    )
    b_recv[me] = b_send[me]
    arrive(b_recv.at[pl.ds(0, n_dev - 1)], recv_sems.at[1])
    wo_ships.append(
        ship(wo_hbm, wo.at[my_tp], 0, 1, wo_send_sems.at[2], wo_recv_sems.at[2])
    )
    q_parts, k_parts, v_parts = [], [], []
    for t in range(tp_size):
        total = b_recv[t].astype(F32)
        for e in range(1, ep_size):
            total = total + b_recv[e * tp_size + t].astype(F32)
        q_parts.append(total[0:q_rows])
        key_row = total[q_rows : q_rows + 1].astype(BF16)
        value_row = total[q_rows + 1 : q_rows + 2].astype(BF16)
        nk_ref[:, t * LANES : (t + 1) * LANES] = key_row
        nv_ref[:, t * LANES : (t + 1) * LANES] = value_row
        k_parts.append(key_row.astype(F32))
        v_parts.append(value_row.astype(F32))
    q_all = jnp.concatenate(q_parts, axis=0).astype(BF16)

    for i in range(5, 9):
        loads[i].wait()
    rows = 2 * repeat
    length = len_s[0]
    positions = kc.shape[0]
    first_map = lax.rem(lax.broadcasted_iota(jnp.int32, (rows, LANES), 0), 2) == 0
    first_wide = lax.rem(lax.broadcasted_iota(jnp.int32, (rows, positions), 0), 2) == 0
    valid = lax.broadcasted_iota(jnp.int32, (rows, positions), 1) < length
    head_at = lax.broadcasted_iota(jnp.int32, (rows, LANES), 0) // 2
    scale = HEAD_QK ** (-0.5)
    contract = (((1,), (1,)), ((), ()))
    for g in range(KV_HEADS):
        q = q_all[g * rows : (g + 1) * rows]
        base = g * 2 * HEAD_QK
        s0 = lax.dot_general(
            q, kc[:, base : base + HEAD_QK], contract, preferred_element_type=F32
        )
        s1 = lax.dot_general(
            q, kc[:, base + HEAD_QK : base + 2 * HEAD_QK], contract, preferred_element_type=F32
        )
        score = jnp.where(valid, jnp.where(first_wide, s0, s1) * scale, -jnp.inf)
        q32 = q.astype(F32)
        own = jnp.sum(
            q32 * jnp.where(first_map, k_parts[2 * g], k_parts[2 * g + 1]), axis=-1, keepdims=True
        ) * scale
        peak = jnp.maximum(jnp.max(score, axis=-1, keepdims=True), own)
        weight = jnp.exp(score - peak)
        own_weight = jnp.exp(own - peak)
        norm = jnp.sum(weight, axis=-1, keepdims=True) + own_weight
        weight = weight / norm
        own_weight = jnp.broadcast_to(own_weight / norm, (rows, LANES))
        lam = jnp.zeros((rows, LANES), F32)
        for r in range(repeat):
            lam = jnp.where(head_at == r, lam_s[g * repeat + r], lam)
        mix = (weight - lam[:, 0:1] * pltpu.roll(weight, rows - 1, 0)).astype(BF16)
        mix_own = (own_weight - lam * pltpu.roll(own_weight, rows - 1, 0)).astype(BF16).astype(F32)
        raw = jnp.dot(
            mix, vc[:, g * HEAD_V : (g + 1) * HEAD_V], preferred_element_type=F32
        )
        raw = raw + jnp.concatenate(
            [mix_own * v_parts[2 * g], mix_own * v_parts[2 * g + 1]], axis=1
        )
        mean_sq = jnp.mean(raw * raw, axis=-1, keepdims=True)
        head = raw * lax.rsqrt(mean_sq + HEAD_EPS) * head_gain[...] * HEAD_SCALE
        c_send[g * rows : (g + 1) * rows, :] = jnp.where(
            first_map, head[:, 0:LANES], pltpu.roll(head[:, LANES : 2 * LANES], 1, 0)
        ).astype(BF16)
    for i, j in ep_peers:
        ship(c_send, c_recv.at[my_ep], i, j, send_sems.at[2], recv_sems.at[2])
    c_recv[my_ep] = c_send[...]
    for half in range(2):
        block = wo.at[tp_of[2], pl.ds(half * rows_half, rows_half)]
        arrive(block, wo_recv_sems.at[half])
        wo_ships.append(
            ship(block, block, 0, 1, wo_send_sems.at[3 + half], wo_recv_sems.at[3 + half])
        )
    loads[9].wait()
    arrive(wo.at[tp_of[1]], wo_recv_sems.at[2])
    for half in range(2):
        block = wo.at[tp_of[3], pl.ds(half * rows_half, rows_half)]
        arrive(block, wo_recv_sems.at[3 + half])
    loads[10].wait()
    arrive(c_recv.at[pl.ds(0, ep_size - 1)], recv_sems.at[2])

    head_rows = c_send.shape[0]
    stage[0 : seq_ep * head_rows, :] = c_recv[...].astype(F32).reshape(seq_ep * head_rows, LANES)
    lhs = jnp.concatenate(
        [stage[pl.ds(r, seq_ep, stride=head_rows), :] for r in range(head_rows)], axis=1
    ).astype(BF16)
    k_block = wo.shape[1]
    total = raw_keep[...]
    for t in range(tp_size):
        total = total + jnp.dot(
            lhs[:, t * k_block : (t + 1) * k_block], wo[t], preferred_element_type=F32
        )
    r_send[...] = total.astype(BF16)
    for i, j in everyone:
        ship(r_send, r_recv.at[my_ep, my_tp], i, j, send_sems.at[3], block_sems.at[i // 2])
    r_recv[my_ep, my_tp] = r_send[...]

    loads[13].wait()
    loads[14].wait()
    square = jnp.zeros((n_dev, LANES), F32)
    for k in range(ep_size // 2):
        arrive(e_recv.at[pl.ds(0, 2 * tp_size if k else 2 * tp_size - 1)], block_sems.at[k])
        gate_add = None
        for i in (2 * k, 2 * k + 1):
            at = pl.multiple_of(ep_of[i] * feat, feat)
            block = r_recv[ep_of[i]].astype(F32).reshape(n_dev, feat)
            for p in range(pieces):
                part = block[:, p * LANES : (p + 1) * LANES]
                square = square + part * part
            scaled = (block * ffn_gain[:, pl.ds(at, feat)]).astype(BF16)
            g_part = jnp.dot(scaled, wg[pl.ds(at, feat), :], preferred_element_type=F32)
            u_part = jnp.dot(scaled, wu[pl.ds(at, feat), :], preferred_element_type=F32)
            gate_add = g_part if gate_add is None else gate_add + g_part
            up_add = u_part if i == 2 * k else up_add + u_part
        if k == 0:
            gate_acc[...] = gate_add
            up_acc[...] = up_add
        elif k < ep_size // 2 - 1:
            gate_acc[...] += gate_add
            up_acc[...] += up_add
    row_scale = lax.rsqrt(jnp.sum(square, axis=-1, keepdims=True) * (1.0 / width) + NORM_EPS)
    gate = (gate_acc[...] + gate_add) * row_scale
    up = (up_acc[...] + up_add) * row_scale
    hidden = (gate / (1.0 + jnp.exp(-gate)) * up).astype(BF16)
    loads[15].wait()
    down = jnp.dot(hidden, wd[...], preferred_element_type=F32)
    for j in range(tile_rows):
        stage[pl.ds(j, n_dev, stride=tile_rows), :] = down[:, j * LANES : (j + 1) * LANES]
    e_send[...] = stage[...].astype(BF16).reshape(tp_size, ep_size, tile_rows, LANES)
    for i, j in everyone:
        ship(
            e_send.at[tp_of[j], ep_of[i]], e_recv.at[me], i, j, send_sems.at[4], recv_sems.at[3]
        )
    e_recv[me] = e_send[my_tp, my_ep]
    loads[11].wait()
    loads[12].wait()
    own_rows = []
    for e in range(ep_size):
        for p in range(pieces):
            own_rows.append((e, p))
    for e, p in own_rows:
        block = r_recv[e, my_tp].astype(F32)
        stage[e * 8 : e * 8 + 8, :] = block[:, 0:LANES]
        stage[(ep_size + e) * 8 : (ep_size + e) * 8 + 8, :] = block[:, LANES : 2 * LANES]
    result = [
        stage[pl.ds((half * ep_size) * 8 + my_ep, ep_size, stride=8), :] for half in range(pieces)
    ]
    for half in range(pieces):
        stage[pl.ds(256 + half, ep_size, stride=pieces), :] = result[half]
    result = stage[256 : 256 + tile_rows, :]
    shares = []
    for e in range(ep_size):
        share = jnp.float32(0.0)
        for k in range(TOPK):
            share = share + jnp.where(routing_s[k, my_tp] == e, rweight_s[k, my_tp], 0.0)
        shares.append(share)
    for ship_done in wo_ships:
        ship_done.wait_send()
    for phase, part in (
        (0, a_recv.at[pl.ds(0, n_dev - 1)]),
        (1, b_recv.at[pl.ds(0, n_dev - 1)]),
        (2, c_recv.at[pl.ds(0, ep_size - 1)]),
    ):
        arrive(part, send_sems.at[phase])
    arrive(e_recv.at[pl.ds(0, n_dev - 1)], send_sems.at[3])
    arrive(e_recv.at[pl.ds(0, n_dev - 1)], recv_sems.at[3])
    for e in range(ep_size):
        total = e_recv[e * tp_size].astype(F32)
        for t in range(1, tp_size):
            total = total + e_recv[e * tp_size + t].astype(F32)
        result = result + total.astype(BF16).astype(F32) * shares[e]
    for j in range(tile_rows):
        out_ref[:, j * LANES : (j + 1) * LANES] = result[j : j + 1].astype(BF16)
    arrive(e_recv.at[pl.ds(0, n_dev - 1)], send_sems.at[4])


def fused_body(
    tokens,
    norm_gain,
    w_query,
    w_key,
    w_value,
    key_cache,
    value_cache,
    lengths,
    diff_lambda,
    head_gain,
    w_out,
    ffn_gain,
    routing,
    route_weight,
    w_gate,
    w_up,
    w_down,
):
    ep_size, tp_size = lax.axis_size("ep"), lax.axis_size("tp")
    n_dev = ep_size * tp_size
    width = tokens.shape[1]
    feat = width // ep_size
    vmem = pl.BlockSpec(memory_space=pltpu.VMEM)
    hbm = pl.BlockSpec(memory_space=pltpu.HBM)
    tile_rows = width // LANES
    proj_cols = w_query.shape[1] + w_key.shape[1] + w_value.shape[1]
    head_tiles = HEADS * HEAD_V // LANES
    scratch = [
        pltpu.VMEM(tokens.shape, BF16),
        pltpu.VMEM((1, width), F32),
        pltpu.VMEM((1, HEAD_V), F32),
        pltpu.VMEM((1, width), F32),
        pltpu.SMEM(diff_lambda.shape, F32),
        pltpu.SMEM(routing.shape[::-1], jnp.int32),
        pltpu.SMEM(route_weight.shape[::-1], F32),
        pltpu.VMEM((feat, proj_cols), BF16),
        pltpu.VMEM(key_cache.shape[1:], BF16),
        pltpu.VMEM(value_cache.shape[1:], BF16),
        pltpu.VMEM((tp_size,) + w_out.shape, BF16),
        pltpu.VMEM(w_gate.shape[1:], BF16),
        pltpu.VMEM(w_up.shape[1:], BF16),
        pltpu.VMEM(w_down.shape[1:], BF16),
        pltpu.VMEM((ep_size, 8, LANES), BF16),
        pltpu.VMEM((n_dev, 8, LANES), BF16),
        pltpu.VMEM((n_dev, 16, LANES), BF16),
        pltpu.VMEM((n_dev, 16, LANES), BF16),
        pltpu.VMEM((head_tiles, LANES), BF16),
        pltpu.VMEM((ep_size, head_tiles, LANES), BF16),
        pltpu.VMEM((ep_size, feat), BF16),
        pltpu.VMEM((ep_size, tp_size, ep_size, feat), BF16),
        pltpu.VMEM((tp_size, ep_size, tile_rows, LANES), BF16),
        pltpu.VMEM((n_dev, tile_rows, LANES), BF16),
        pltpu.VMEM((n_dev * 16, LANES), F32),
        pltpu.VMEM((ep_size, feat), F32),
        pltpu.VMEM((n_dev, w_gate.shape[2]), F32),
        pltpu.VMEM((n_dev, w_gate.shape[2]), F32),
        pltpu.SemaphoreType.DMA((16,)),
        pltpu.SemaphoreType.DMA((5,)),
        pltpu.SemaphoreType.DMA((4,)),
        pltpu.SemaphoreType.DMA((ep_size // 2,)),
        pltpu.SemaphoreType.DMA((5,)),
        pltpu.SemaphoreType.DMA((5,)),
    ]
    call = pl.pallas_call(
        functools.partial(fused_kernel, ep_size, tp_size),
        name="fused_layer",
        out_shape=(
            jax.ShapeDtypeStruct(tokens.shape, BF16),
            jax.ShapeDtypeStruct((1, key_cache.shape[2]), BF16),
            jax.ShapeDtypeStruct((1, value_cache.shape[2]), BF16),
        ),
        in_specs=[hbm] * 7 + [pl.BlockSpec(memory_space=pltpu.SMEM)] + [hbm] * 9,
        out_specs=(vmem, vmem, vmem),
        scratch_shapes=scratch,
        compiler_params=pltpu.CompilerParams(
            collective_id=0, has_side_effects=True, vmem_limit_bytes=28 * 1024 * 1024
        ),
    )
    operands = (
        tokens,
        norm_gain.reshape(1, -1),
        w_query,
        w_key,
        w_value,
        key_cache,
        value_cache,
        lengths,
        diff_lambda,
        head_gain.reshape(1, -1),
        w_out,
        ffn_gain.reshape(1, -1),
        routing.T,
        route_weight.T,
        w_gate,
        w_up,
        w_down,
    )
    pinned = [
        array if array is lengths else pltpu.with_memory_space_constraint(array, pltpu.HBM)
        for array in operands
    ]
    return call(*pinned)


def layer(*arrays):
    tokens, w_query, w_key = arrays[0], arrays[2], arrays[3]
    feat = tokens.shape[1] // lax.axis_size("ep")
    whole_tiles = (
        tokens.shape[0] == 1
        and w_key.shape[1] == LANES
        and w_query.shape[1] == 8 * LANES
        and feat == 2 * LANES
        and tokens.shape[1] == 16 * LANES
    )
    return fused_body(*arrays) if whole_tiles else body(*arrays)


def solution(mesh):
    placed = (
        P(("ep", "tp"), None),
        P(),
        P("ep", "tp"),
        P("ep", "tp"),
        P("ep", "tp"),
        P(("ep", "tp"), None, None),
        P(("ep", "tp"), None, None),
        P(("ep", "tp")),
        P(),
        P(),
        P("tp", "ep"),
        P(),
        P("ep", None),
        P("ep", None),
        P("ep", None, "tp"),
        P("ep", None, "tp"),
        P("ep", "tp", None),
    )
    return jax.shard_map(
        layer,
        mesh=mesh,
        in_specs=placed,
        out_specs=(P(("ep", "tp"), None), P(("ep", "tp"), None), P(("ep", "tp"), None)),
        check_vma=False,
    )
```

```python
import functools

import jax
import jax.numpy as jnp
from jax import lax
from jax.experimental import pallas as pl
from jax.experimental.pallas import tpu as pltpu
from jax.sharding import PartitionSpec as P

HEADS = 16
KV_HEADS = 2
HEAD_QK = 128
HEAD_V = 256
TOPK = 2
LEN = 1024
SEQ_DEV = 1


NORM_EPS = 1e-05
HEAD_EPS = 0.01
HEAD_SCALE = 0.8


def rms_scale(values, gain_row, floor_add):
    mean_sq = jnp.mean(values * values, axis=-1, keepdims=True)
    return values * lax.rsqrt(mean_sq + floor_add) * gain_row


def attend(queries, key_rows, value_rows, key_cache, value_cache, lengths, diff_lambda, head_gain):
    row_count = queries.shape[0]
    repeat = HEADS // KV_HEADS
    queries = queries.reshape(row_count, KV_HEADS, repeat, 2, HEAD_QK)
    key_rows = key_rows.reshape(row_count, KV_HEADS, 2, HEAD_QK)
    value_rows = value_rows.reshape(row_count, KV_HEADS, HEAD_V)
    cache_keys = key_cache.reshape(row_count, LEN, KV_HEADS, 2, HEAD_QK)
    cache_vals = value_cache.reshape(row_count, LEN, KV_HEADS, HEAD_V)
    score_scale = HEAD_QK ** (-0.5)
    cached = (
        jnp.einsum("sgrcd,slgcd->sgrcl", queries, cache_keys, preferred_element_type=jnp.float32)
        * score_scale
    )
    own_score = (
        jnp.einsum("sgrcd,sgcd->sgrc", queries, key_rows, preferred_element_type=jnp.float32)
        * score_scale
    )
    in_range = jnp.arange(LEN)[None, :] < lengths[:, None]
    cached = jnp.where(in_range[:, None, None, None, :], cached, -jnp.inf)
    row_peak = jnp.maximum(jnp.max(cached, axis=-1), own_score)
    cached_w = jnp.exp(cached - row_peak[..., None])
    own_w = jnp.exp(own_score - row_peak)
    row_total = jnp.sum(cached_w, axis=-1) + own_w
    cached_w = cached_w / row_total[..., None]
    own_w = own_w / row_total
    lam_heads = diff_lambda.reshape(1, KV_HEADS, repeat)
    mix_cached = (cached_w[:, :, :, 0] - lam_heads[..., None] * cached_w[:, :, :, 1]).astype(
        jnp.bfloat16
    )
    mix_own = (own_w[..., 0] - lam_heads * own_w[..., 1]).astype(jnp.bfloat16)
    head_raw = jnp.einsum(
        "sgrl,slgv->sgrv", mix_cached, cache_vals, preferred_element_type=jnp.float32
    )
    head_raw = (
        head_raw
        + mix_own.astype(jnp.float32)[..., None] * value_rows.astype(jnp.float32)[:, :, None, :]
    )
    head_out = rms_scale(head_raw, head_gain, HEAD_EPS) * HEAD_SCALE
    return head_out.astype(jnp.bfloat16).reshape(row_count, HEADS * HEAD_V)


def body(
    tokens,
    norm_gain,
    w_query,
    w_key,
    w_value,
    key_cache,
    value_cache,
    lengths,
    diff_lambda,
    head_gain,
    w_out,
    ffn_gain,
    routing,
    route_weight,
    w_gate,
    w_up,
    w_down,
):
    group_tokens = lax.all_gather(tokens, "tp", axis=0, tiled=True)
    normed = rms_scale(group_tokens.astype(jnp.float32), norm_gain, NORM_EPS).astype(jnp.bfloat16)
    blocks = lax.all_to_all(normed, "ep", split_axis=1, concat_axis=0, tiled=True)
    query_term = jnp.dot(blocks, w_query, preferred_element_type=jnp.float32)
    key_term = jnp.dot(blocks, w_key, preferred_element_type=jnp.float32)
    value_term = jnp.dot(blocks, w_value, preferred_element_type=jnp.float32)
    query_sum, key_sum, value_sum = (
        lax.psum_scatter(query_term, "ep", scatter_dimension=0, tiled=True),
        lax.psum_scatter(key_term, "ep", scatter_dimension=0, tiled=True),
        lax.psum_scatter(value_term, "ep", scatter_dimension=0, tiled=True),
    )
    queries = query_sum.astype(jnp.bfloat16)
    keys_made = key_sum.astype(jnp.bfloat16)
    values_made = value_sum.astype(jnp.bfloat16)
    own_query, new_keys, new_values = (
        lax.all_to_all(queries, "tp", split_axis=0, concat_axis=1, tiled=True),
        lax.all_to_all(keys_made, "tp", split_axis=0, concat_axis=1, tiled=True),
        lax.all_to_all(values_made, "tp", split_axis=0, concat_axis=1, tiled=True),
    )
    head_out = attend(
        own_query, new_keys, new_values, key_cache, value_cache, lengths, diff_lambda, head_gain
    )
    head_rows = lax.all_to_all(head_out, "tp", split_axis=1, concat_axis=0, tiled=True)
    partial_out = jnp.dot(
        head_rows,
        lax.all_gather(w_out, "ep", axis=1, tiled=True),
        preferred_element_type=jnp.float32,
    )
    attn_sum = lax.psum_scatter(
        partial_out.astype(jnp.bfloat16), "tp", scatter_dimension=0, tiled=True
    ).astype(jnp.float32)
    residual = tokens.astype(jnp.float32) + attn_sum
    ffn_in = rms_scale(residual, ffn_gain, NORM_EPS).astype(jnp.bfloat16)
    group_in = lax.all_gather(ffn_in, "tp", axis=0, tiled=True)
    experts = lax.axis_size("ep")
    capacity = 8 * SEQ_DEV * lax.axis_size("tp") // experts
    group_rows = group_in.shape[0]
    picks = routing.reshape(-1)
    choose = (picks[:, None] == jnp.arange(experts)[None, :]).astype(jnp.int32)
    earlier = jnp.cumsum(choose, axis=0) - choose
    slot_in = jnp.sum(earlier * choose, axis=1)
    slot_ids = (picks * capacity + slot_in).reshape(group_rows, TOPK)
    slot_hit = slot_ids[:, :, None] == jnp.arange(experts * capacity)[None, None, :]
    dispatch = jnp.sum(slot_hit, axis=1).astype(jnp.bfloat16)
    outgoing = jnp.einsum(
        "rj,rd->jd", dispatch, group_in, preferred_element_type=jnp.float32
    ).astype(jnp.bfloat16)
    outgoing = outgoing.reshape(experts, capacity, group_in.shape[1])
    arrived = lax.all_to_all(outgoing, "ep", split_axis=0, concat_axis=0, tiled=True)
    sources, slot_count, feat_dim = arrived.shape
    flat_rows = arrived.reshape(sources * slot_count, feat_dim)
    gate_pre = jnp.dot(flat_rows, w_gate[0], preferred_element_type=jnp.float32)
    up_pre = jnp.dot(flat_rows, w_up[0], preferred_element_type=jnp.float32)
    hidden = (jax.nn.silu(gate_pre) * up_pre).astype(jnp.bfloat16)
    partial_down = jnp.dot(hidden, w_down[0], preferred_element_type=jnp.float32)
    summed = lax.psum_scatter(
        partial_down.astype(jnp.bfloat16), "tp", scatter_dimension=1, tiled=True
    )
    expert_rows = summed.reshape(sources, slot_count, summed.shape[1])
    returned = lax.all_to_all(expert_rows, "ep", split_axis=0, concat_axis=0, tiled=True)
    combine = jnp.sum(slot_hit.astype(jnp.float32) * route_weight[:, :, None], axis=1)
    flat_back = returned.reshape(experts * capacity, returned.shape[2]).astype(jnp.float32)
    moe_cols = jnp.dot(combine, flat_back, precision=lax.Precision.HIGHEST)
    moe_own = lax.all_to_all(moe_cols, "tp", split_axis=0, concat_axis=1, tiled=True)
    return ((residual + moe_own).astype(jnp.bfloat16), new_keys, new_values)


F32 = jnp.float32
BF16 = jnp.bfloat16
LANES = 128


WO_CUTS = (4, 4)
WO_FIRST = 1


def fused_kernel(
    ep_size,
    tp_size,
    tok_hbm,
    norm_gain_hbm,
    wq_hbm,
    wk_hbm,
    wv_hbm,
    kc_hbm,
    vc_hbm,
    len_s,
    lam_hbm,
    head_gain_hbm,
    wo_hbm,
    ffn_gain_hbm,
    routing_hbm,
    rweight_hbm,
    wg_hbm,
    wu_hbm,
    wd_hbm,
    out_ref,
    nk_ref,
    nv_ref,
    tok_v,
    norm_gain,
    head_gain,
    ffn_gain,
    lam_s,
    routing_s,
    rweight_s,
    wqkv,
    kc,
    kt,
    vc,
    wo,
    wg,
    wu,
    wd,
    a_send,
    a_recv,
    b_send,
    b_recv,
    c_send,
    c_recv,
    r_send,
    r_recv,
    e_send,
    e_recv,
    stage,
    raw_keep,
    gate_acc,
    up_acc,
    load_sems,
    send_sems,
    recv_sems,
    block_sems,
    wo_send_sems,
    wo_recv_sems,
):
    n_dev = ep_size * tp_size
    my_ep = lax.axis_index("ep")
    my_tp = lax.axis_index("tp")
    me = my_ep * tp_size + my_tp
    my_row, my_col = my_tp // 2, lax.rem(my_tp, 2)
    other_col = 1 - my_col
    my_slot = my_ep * 2 + my_row
    slots = 2 * ep_size
    width = tok_v.shape[1]
    feat = width // ep_size
    pieces = feat // LANES
    q_cols = wq_hbm.shape[1]
    q_rows = q_cols // LANES
    repeat = HEADS // KV_HEADS
    tile_rows = width // LANES
    a_rows = a_send.shape[1]
    b_tiles, b_rows = b_send.shape[1:3]
    b_span = b_tiles * b_rows

    def flips(index, size):
        bits = [lax.rem(index // (1 << b), 2) for b in range(size.bit_length() - 1)]
        return [
            sum(
                ((1 - bit) if (mask >> b) & 1 else bit) * (1 << b)
                for b, bit in enumerate(bits)
            )
            for mask in range(size)
        ]

    ep_of = flips(my_ep, ep_size)
    tp_of = flips(my_tp, tp_size)
    everyone = [
        (i, j) for i in reversed(range(ep_size)) for j in reversed(range(tp_size)) if i or j
    ]
    spread = sorted(everyone, key=lambda peer: -((peer[0] // 2) ^ (peer[0] // 4)))
    cross = [(i, j) for i in reversed(range(ep_size)) for j in (3, 1)]

    barrier = pltpu.get_barrier_semaphore()
    for i, j in everyone:
        pl.semaphore_signal(
            barrier,
            inc=1,
            device_id={"ep": ep_of[i], "tp": tp_of[j]},
            device_id_type=pl.DeviceIdType.MESH,
        )

    wo_rows = wo_hbm.shape[0]
    near_cols = pl.ds(pl.multiple_of(my_row * LANES, LANES), LANES)
    far_cols = pl.ds(pl.multiple_of((1 - my_row) * LANES, LANES), LANES)
    cuts = [wo_rows * eighths // 8 for eighths in WO_CUTS]
    spans = [pl.ds(sum(cuts[:n]), count) for n, count in enumerate(cuts)]
    wo_ships = []

    def wo_push(n):
        wo_ships.append(
            ship(
                wo_hbm.at[spans[n], far_cols],
                wo.at[my_tp, spans[n]],
                0,
                2,
                wo_send_sems.at[n],
                wo_recv_sems.at[n],
            )
        )

    def wo_forward(n):
        at = len(cuts) + 1 + n
        block = wo.at[tp_of[2], spans[n]]
        arrive(block, wo_recv_sems.at[n])
        wo_ships.append(ship(block, block, 0, 1, wo_send_sems.at[at], wo_recv_sems.at[at]))

    load_list = [
        (tok_hbm, tok_v),
        (norm_gain_hbm, norm_gain),
        (wq_hbm, wqkv.at[my_col, :, pl.ds(0, q_cols)]),
        (wk_hbm, wqkv.at[my_col, :, pl.ds(q_cols, LANES)]),
        (wv_hbm, wqkv.at[my_col, :, pl.ds(q_cols + LANES, LANES)]),
        (kc_hbm.at[0], kc),
        (vc_hbm.at[0], vc),
        (lam_hbm, lam_s),
        (head_gain_hbm, head_gain),
        (wo_hbm.at[:, near_cols], wo.at[my_tp]),
        (ffn_gain_hbm, ffn_gain),
        (routing_hbm, routing_s),
        (rweight_hbm, rweight_s),
        (wg_hbm.at[0], wg),
        (wu_hbm.at[0], wu),
        (wd_hbm.at[0], wd),
    ]
    loads = [
        pltpu.make_async_copy(src, dst, load_sems.at[i]) for i, (src, dst) in enumerate(load_list)
    ]
    for load in loads:
        load.start()

    def ship(src, dst, i, j, send_sem, recv_sem):
        copy = pltpu.make_async_remote_copy(
            src_ref=src,
            dst_ref=dst,
            send_sem=send_sem,
            recv_sem=recv_sem,
            device_id={"ep": ep_of[i], "tp": tp_of[j]},
            device_id_type=pl.DeviceIdType.MESH,
        )
        copy.start()
        return copy

    def arrive(target, sem):
        pltpu.make_async_copy(target, target, sem).wait()

    loads[0].wait()
    loads[1].wait()
    tok = tok_v[...].astype(F32)
    mean_sq = jnp.mean(tok * tok, axis=-1, keepdims=True)
    normed = tok * lax.rsqrt(mean_sq + NORM_EPS) * norm_gain[...]
    for e in range(ep_size):
        for p in range(pieces):
            cols = slice(e * feat + p * LANES, e * feat + (p + 1) * LANES)
            at = e * a_rows + p
            stage[at : at + 1, :] = normed[:, cols]
            stage[at + pieces : at + pieces + 1, :] = tok[:, cols]
    for e in range(ep_size):
        a_send[e] = stage[e * a_rows : (e + 1) * a_rows, :].astype(BF16)
    pl.semaphore_wait(barrier, n_dev - 1)
    for i, j in cross:
        ship(a_send.at[ep_of[i]], a_recv.at[my_slot], i, j, send_sems.at[0], recv_sems.at[0])
    pair_ships = [
        ship(
            src,
            wqkv.at[my_col, :, pl.ds(first, src.shape[1])],
            0,
            1,
            wo_send_sems.at[2 * len(cuts) + 1 + n],
            wo_recv_sems.at[2 * len(cuts) + 1 + n],
        )
        for n, (src, first) in enumerate(
            ((wq_hbm, 0), (wk_hbm, q_cols), (wv_hbm, q_cols + LANES))
        )
    ]
    for n in range(WO_FIRST):
        wo_push(n)
    arrive(a_recv, recv_sems.at[0])
    for n in range(slots):
        stage[n * a_rows : (n + 1) * a_rows, :] = a_recv[n].astype(F32)
    blocks = jnp.concatenate(
        [stage[pl.ds(p, slots, stride=a_rows), :] for p in range(pieces)], axis=1
    ).astype(BF16)
    raw_keep[...] = stage[pl.ds(pieces + my_row, slots, stride=a_rows), :]

    for i in range(2, 5):
        loads[i].wait()
    for n, (first, count) in enumerate(((0, q_cols), (q_cols, LANES), (q_cols + LANES, LANES))):
        arrive(
            wqkv.at[other_col, :, pl.ds(first, count)], wo_recv_sems.at[2 * len(cuts) + 1 + n]
        )
    for col in range(2):
        proj = jnp.dot(blocks, wqkv[col], preferred_element_type=F32)
        rows_at = [col * q_rows + j for j in range(q_rows)] + [2 * q_rows + col, 2 * q_rows + 2 + col]
        for j, at in enumerate(rows_at):
            stage[pl.ds(at, slots, stride=b_span), :] = proj[:, j * LANES : (j + 1) * LANES]
    for n in range(slots):
        for k in range(b_tiles):
            at = n * b_span + k * b_rows
            b_send[n, k] = stage[at : at + b_rows, :].astype(BF16)
    for i, j in cross:
        to = ep_of[i] * 2 + tp_of[j] // 2
        ship(b_send.at[to], b_recv.at[my_slot], i, j, send_sems.at[1], recv_sems.at[1])
    for n in range(WO_FIRST, len(cuts)):
        wo_push(n)
    wo_ships.append(
        ship(
            wo_hbm.at[:, near_cols],
            wo.at[my_tp],
            0,
            1,
            wo_send_sems.at[len(cuts)],
            wo_recv_sems.at[len(cuts)],
        )
    )
    loads[5].wait()
    for part in range(kc.shape[1] // HEAD_QK):
        cols = slice(part * HEAD_QK, (part + 1) * HEAD_QK)
        kt[cols, :] = kc[:, cols].T
    arrive(b_recv, recv_sems.at[1])
    for n in range(WO_FIRST):
        wo_forward(n)
    k_parts, v_parts = [], []
    for row in range(2):
        total = b_recv[row].astype(F32)
        for e in range(1, ep_size):
            total = total + b_recv[e * 2 + row].astype(F32)
        for k in range(2 * q_rows // b_rows):
            at = row * 2 * q_rows + k * b_rows
            stage[at : at + b_rows, :] = total[k]
        for col in range(2):
            t = row * 2 + col
            key_row = total[b_tiles - 1, col : col + 1].astype(BF16)
            value_row = total[b_tiles - 1, 2 + col : 3 + col].astype(BF16)
            nk_ref[:, t * LANES : (t + 1) * LANES] = key_row
            nv_ref[:, t * LANES : (t + 1) * LANES] = value_row
            k_parts.append(key_row.astype(F32))
            v_parts.append(value_row.astype(F32))
    q_all = stage[0 : tp_size * q_rows, :].astype(BF16)

    for i in range(6, 9):
        loads[i].wait()
    rows = 2 * repeat
    length = len_s[0]
    positions = kc.shape[0]
    first_map = lax.rem(lax.broadcasted_iota(jnp.int32, (rows, LANES), 0), 2) == 0
    valid = lax.broadcasted_iota(jnp.int32, (rows, positions), 1) < length
    head_at = lax.broadcasted_iota(jnp.int32, (rows, LANES), 0) // 2
    scale = HEAD_QK ** (-0.5)
    for g in range(KV_HEADS):
        q = q_all[g * rows : (g + 1) * rows]
        base = g * 2 * HEAD_QK
        q32 = q.astype(F32)
        both = jnp.concatenate(
            [jnp.where(first_map, q32, 0.0), jnp.where(first_map, 0.0, q32)], axis=1
        ).astype(BF16)
        score = jnp.dot(both, kt[base : base + 2 * HEAD_QK, :], preferred_element_type=F32)
        score = jnp.where(valid, score * scale, -jnp.inf)
        own = jnp.sum(
            q32 * jnp.where(first_map, k_parts[2 * g], k_parts[2 * g + 1]), axis=-1, keepdims=True
        ) * scale
        peak = jnp.maximum(jnp.max(score, axis=-1, keepdims=True), own)
        weight = jnp.exp(score - peak)
        own_weight = jnp.exp(own - peak)
        norm = jnp.sum(weight, axis=-1, keepdims=True) + own_weight
        weight = weight / norm
        own_weight = jnp.broadcast_to(own_weight / norm, (rows, LANES))
        lam = jnp.zeros((rows, LANES), F32)
        for r in range(repeat):
            lam = jnp.where(head_at == r, lam_s[g * repeat + r], lam)
        mix = (weight - lam[:, 0:1] * pltpu.roll(weight, rows - 1, 0)).astype(BF16)
        mix_own = (own_weight - lam * pltpu.roll(own_weight, rows - 1, 0)).astype(BF16).astype(F32)
        raw = jnp.dot(
            mix, vc[:, g * HEAD_V : (g + 1) * HEAD_V], preferred_element_type=F32
        )
        raw = raw + jnp.concatenate(
            [mix_own * v_parts[2 * g], mix_own * v_parts[2 * g + 1]], axis=1
        )
        mean_sq = jnp.mean(raw * raw, axis=-1, keepdims=True)
        head = raw * lax.rsqrt(mean_sq + HEAD_EPS) * head_gain[...] * HEAD_SCALE
        c_send[g * rows : (g + 1) * rows, :] = jnp.where(
            first_map, head[:, 0:LANES], pltpu.roll(head[:, LANES : 2 * LANES], 1, 0)
        ).astype(BF16)
    for i, j in cross:
        ship(c_send, c_recv.at[my_slot], i, j, send_sems.at[2], recv_sems.at[2])
    for n in range(WO_FIRST, len(cuts)):
        wo_forward(n)
    loads[9].wait()
    loads[10].wait()
    arrive(wo.at[tp_of[1]], wo_recv_sems.at[len(cuts)])
    for n in range(len(cuts)):
        arrive(wo.at[tp_of[3], spans[n]], wo_recv_sems.at[len(cuts) + 1 + n])
    arrive(c_recv, recv_sems.at[2])

    head_rows = c_send.shape[0]
    tiles_block = head_rows // tp_size
    for n in range(slots):
        part = c_recv[n].astype(F32)
        for t in range(tp_size):
            at = (t * slots + n) * tiles_block
            stage[at : at + tiles_block, :] = part[t * tiles_block : (t + 1) * tiles_block]

    total = raw_keep[...]
    for t in range(tp_size):
        lhs = jnp.concatenate(
            [
                stage[pl.ds(t * tiles_block * slots + r, slots, stride=tiles_block), :]
                for r in range(tiles_block)
            ],
            axis=1,
        ).astype(BF16)
        total = total + jnp.dot(lhs, wo[t], preferred_element_type=F32)
    r_send[...] = total.astype(BF16)
    for i, j in spread:
        ship(r_send, r_recv.at[my_ep, my_tp], i, j, send_sems.at[3], block_sems.at[i])
    r_recv[my_ep, my_tp] = r_send[...]

    loads[13].wait()
    loads[14].wait()
    low, high = lax.rem(my_ep // 2, 2), my_ep // 4
    inner = low + high - 2 * low * high
    order = [(at_end, inside) for at_end, inside in zip((1, 0, 3, 2, 5, 4, 7, 6), (1, 0, 7, 6, 3, 2, 5, 4))]

    def pick(at_end, inside):
        return inside * inner + at_end * (1 - inner)

    square = jnp.zeros((n_dev, LANES), F32)
    for step, (at_end, inside) in enumerate(order):
        place = pick(ep_of[at_end], ep_of[inside])
        count = tp_size if at_end else tp_size - 1
        arrive(r_recv.at[place, pl.ds(0, count)], block_sems.at[pick(at_end, inside)])
        at = pl.multiple_of(place * feat, feat)
        parts = []
        for p in range(pieces):
            part = r_recv[place, 2 * p : 2 * p + 2].astype(F32).reshape(n_dev, LANES)
            square = square + part * part
            parts.append(part * ffn_gain[:, pl.ds(at + p * LANES, LANES)])
        scaled = jnp.concatenate(parts, axis=1).astype(BF16)
        gate_add = jnp.dot(scaled, wg[pl.ds(at, feat), :], preferred_element_type=F32)
        up_add = jnp.dot(scaled, wu[pl.ds(at, feat), :], preferred_element_type=F32)
        if step == 0:
            gate_acc[...] = gate_add
            up_acc[...] = up_add
        elif step < ep_size - 1:
            gate_acc[...] += gate_add
            up_acc[...] += up_add
    row_scale = lax.rsqrt(jnp.sum(square, axis=-1, keepdims=True) * (1.0 / width) + NORM_EPS)
    gate = (gate_acc[...] + gate_add) * row_scale
    up = (up_acc[...] + up_add) * row_scale
    hidden = (gate / (1.0 + jnp.exp(-gate)) * up).astype(BF16)
    loads[15].wait()

    def row_of(e, t):
        return (1 - lax.rem(t, 2)) * slots + e * 2 + t // 2

    down = jnp.dot(hidden, wd[...], preferred_element_type=F32)
    for j in range(tile_rows):
        stage[pl.ds(j, n_dev, stride=tile_rows), :] = down[:, j * LANES : (j + 1) * LANES]
    e_send[...] = stage[...].astype(BF16).reshape(n_dev, tile_rows, LANES)
    for i, j in spread:
        ship(
            e_send.at[row_of(ep_of[i], tp_of[j])],
            e_recv.at[me],
            i,
            j,
            send_sems.at[4],
            recv_sems.at[3],
        )
    e_recv[me] = e_send[row_of(my_ep, my_tp)]
    loads[11].wait()
    loads[12].wait()
    for e in range(ep_size):
        for p in range(pieces):
            at = (e * pieces + p) * slots
            stage[at : at + slots, :] = r_recv[e, 2 * p + other_col].astype(F32)
    result = stage[pl.ds(my_slot, tile_rows, stride=slots), :]
    shares = []
    for e in range(ep_size):
        share = jnp.float32(0.0)
        for k in range(TOPK):
            share = share + jnp.where(routing_s[k, my_tp] == e, rweight_s[k, my_tp], 0.0)
        shares.append(share)
    for ship_done in wo_ships + pair_ships:
        ship_done.wait_send()
    for phase, part in (
        (0, a_recv),
        (1, b_recv),
        (2, c_recv),
    ):
        arrive(part, send_sems.at[phase])
    arrive(e_recv.at[pl.ds(0, n_dev - 1)], send_sems.at[3])
    arrive(e_recv.at[pl.ds(0, n_dev - 1)], recv_sems.at[3])
    for e in range(ep_size):
        total = e_recv[e * tp_size].astype(F32)
        for t in range(1, tp_size):
            total = total + e_recv[e * tp_size + t].astype(F32)
        result = result + total.astype(BF16).astype(F32) * shares[e]
    for j in range(tile_rows):
        out_ref[:, j * LANES : (j + 1) * LANES] = result[j : j + 1].astype(BF16)
    arrive(e_recv.at[pl.ds(0, n_dev - 1)], send_sems.at[4])


def write_kernel(result_ref, keys_ref, values_ref, result_out, keys_out, values_out, sems):
    copies = [
        pltpu.make_async_copy(src, dst, sems.at[i])
        for i, (src, dst) in enumerate(
            ((result_ref, result_out), (keys_ref, keys_out), (values_ref, values_out))
        )
    ]
    for copy in copies:
        copy.start()
    for copy in copies:
        copy.wait()


def fused_body(
    tokens,
    norm_gain,
    w_query,
    w_key,
    w_value,
    key_cache,
    value_cache,
    lengths,
    diff_lambda,
    head_gain,
    w_out,
    ffn_gain,
    routing,
    route_weight,
    w_gate,
    w_up,
    w_down,
):
    ep_size, tp_size = lax.axis_size("ep"), lax.axis_size("tp")
    n_dev = ep_size * tp_size
    width = tokens.shape[1]
    feat = width // ep_size
    vmem = pl.BlockSpec(memory_space=pltpu.VMEM)
    hbm = pl.BlockSpec(memory_space=pltpu.HBM)
    tile_rows = width // LANES
    proj_cols = w_query.shape[1] + w_key.shape[1] + w_value.shape[1]
    head_tiles = HEADS * HEAD_V // LANES
    scratch = [
        pltpu.VMEM(tokens.shape, BF16),
        pltpu.VMEM((1, width), F32),
        pltpu.VMEM((1, HEAD_V), F32),
        pltpu.VMEM((1, width), F32),
        pltpu.SMEM(diff_lambda.shape, F32),
        pltpu.SMEM(routing.shape[::-1], jnp.int32),
        pltpu.SMEM(route_weight.shape[::-1], F32),
        pltpu.VMEM((2, feat, proj_cols), BF16),
        pltpu.VMEM(key_cache.shape[1:], BF16),
        pltpu.VMEM(key_cache.shape[:0:-1], BF16),
        pltpu.VMEM(value_cache.shape[1:], BF16),
        pltpu.VMEM((tp_size, w_out.shape[0], LANES), BF16),
        pltpu.VMEM(w_gate.shape[1:], BF16),
        pltpu.VMEM(w_up.shape[1:], BF16),
        pltpu.VMEM(w_down.shape[1:], BF16),
        pltpu.VMEM((ep_size, 4, LANES), BF16),
        pltpu.VMEM((2 * ep_size, 4, LANES), BF16),
        pltpu.VMEM((2 * ep_size, 5, 4, LANES), BF16),
        pltpu.VMEM((2 * ep_size, 5, 4, LANES), BF16),
        pltpu.VMEM((head_tiles, LANES), BF16),
        pltpu.VMEM((2 * ep_size, head_tiles, LANES), BF16),
        pltpu.VMEM((2 * ep_size, LANES), BF16),
        pltpu.VMEM((ep_size, tp_size, 2 * ep_size, LANES), BF16),
        pltpu.VMEM((n_dev, tile_rows, LANES), BF16),
        pltpu.VMEM((n_dev, tile_rows, LANES), BF16),
        pltpu.VMEM((n_dev * 16, LANES), F32),
        pltpu.VMEM((2 * ep_size, LANES), F32),
        pltpu.VMEM((n_dev, w_gate.shape[2]), F32),
        pltpu.VMEM((n_dev, w_gate.shape[2]), F32),
        pltpu.SemaphoreType.DMA((16,)),
        pltpu.SemaphoreType.DMA((5,)),
        pltpu.SemaphoreType.DMA((4,)),
        pltpu.SemaphoreType.DMA((ep_size,)),
        pltpu.SemaphoreType.DMA((2 * len(WO_CUTS) + 4,)),
        pltpu.SemaphoreType.DMA((2 * len(WO_CUTS) + 4,)),
    ]
    call = pl.pallas_call(
        functools.partial(fused_kernel, ep_size, tp_size),
        name="fused_layer",
        out_shape=(
            jax.ShapeDtypeStruct(tokens.shape, BF16),
            jax.ShapeDtypeStruct((1, key_cache.shape[2]), BF16),
            jax.ShapeDtypeStruct((1, value_cache.shape[2]), BF16),
        ),
        in_specs=[hbm] * 7 + [pl.BlockSpec(memory_space=pltpu.SMEM)] + [hbm] * 9,
        out_specs=(vmem, vmem, vmem),
        scratch_shapes=scratch,
        compiler_params=pltpu.CompilerParams(
            collective_id=0, has_side_effects=True, vmem_limit_bytes=28 * 1024 * 1024
        ),
    )
    operands = (
        tokens,
        norm_gain.reshape(1, -1),
        w_query,
        w_key,
        w_value,
        key_cache,
        value_cache,
        lengths,
        diff_lambda,
        head_gain.reshape(1, -1),
        w_out,
        ffn_gain.reshape(1, -1),
        routing.T,
        route_weight.T,
        w_gate,
        w_up,
        w_down,
    )
    pinned = [
        array if array is lengths else pltpu.with_memory_space_constraint(array, pltpu.HBM)
        for array in operands
    ]
    made = call(*pinned)
    return pl.pallas_call(
        write_kernel,
        name="write_out",
        out_shape=tuple(jax.ShapeDtypeStruct(array.shape, array.dtype) for array in made),
        in_specs=[vmem] * len(made),
        out_specs=tuple(pl.BlockSpec(memory_space=pl.ANY) for _ in made),
        scratch_shapes=[pltpu.SemaphoreType.DMA((len(made),))],
        compiler_params=pltpu.CompilerParams(vmem_limit_bytes=1024 * 1024),
    )(*made)


def layer(*arrays):
    tokens, w_query, w_key = arrays[0], arrays[2], arrays[3]
    feat = tokens.shape[1] // lax.axis_size("ep")
    whole_tiles = (
        tokens.shape[0] == 1
        and w_key.shape[1] == LANES
        and w_query.shape[1] == 8 * LANES
        and feat == 2 * LANES
        and tokens.shape[1] == 16 * LANES
    )
    return fused_body(*arrays) if whole_tiles else body(*arrays)


def solution(mesh):
    placed = (
        P(("ep", "tp"), None),
        P(),
        P("ep", "tp"),
        P("ep", "tp"),
        P("ep", "tp"),
        P(("ep", "tp"), None, None),
        P(("ep", "tp"), None, None),
        P(("ep", "tp")),
        P(),
        P(),
        P("tp", "ep"),
        P(),
        P("ep", None),
        P("ep", None),
        P("ep", None, "tp"),
        P("ep", None, "tp"),
        P("ep", "tp", None),
    )
    return jax.shard_map(
        layer,
        mesh=mesh,
        in_specs=placed,
        out_specs=(P(("ep", "tp"), None), P(("ep", "tp"), None), P(("ep", "tp"), None)),
        check_vma=False,
    )
```

```python
import functools

import jax
import jax.numpy as jnp
from jax import lax
from jax.experimental import pallas as pl
from jax.experimental.pallas import tpu as pltpu
from jax.sharding import PartitionSpec as P

HEADS = 16
KV_HEADS = 2
HEAD_QK = 128
HEAD_V = 256
TOPK = 2
LEN = 1024
SEQ_DEV = 1


NORM_EPS = 1e-05
HEAD_EPS = 0.01
HEAD_SCALE = 0.8


def rms_scale(values, gain_row, floor_add):
    mean_sq = jnp.mean(values * values, axis=-1, keepdims=True)
    return values * lax.rsqrt(mean_sq + floor_add) * gain_row


def attend(queries, key_rows, value_rows, key_cache, value_cache, lengths, diff_lambda, head_gain):
    row_count = queries.shape[0]
    repeat = HEADS // KV_HEADS
    queries = queries.reshape(row_count, KV_HEADS, repeat, 2, HEAD_QK)
    key_rows = key_rows.reshape(row_count, KV_HEADS, 2, HEAD_QK)
    value_rows = value_rows.reshape(row_count, KV_HEADS, HEAD_V)
    cache_keys = key_cache.reshape(row_count, LEN, KV_HEADS, 2, HEAD_QK)
    cache_vals = value_cache.reshape(row_count, LEN, KV_HEADS, HEAD_V)
    score_scale = HEAD_QK ** (-0.5)
    cached = (
        jnp.einsum("sgrcd,slgcd->sgrcl", queries, cache_keys, preferred_element_type=jnp.float32)
        * score_scale
    )
    own_score = (
        jnp.einsum("sgrcd,sgcd->sgrc", queries, key_rows, preferred_element_type=jnp.float32)
        * score_scale
    )
    in_range = jnp.arange(LEN)[None, :] < lengths[:, None]
    cached = jnp.where(in_range[:, None, None, None, :], cached, -jnp.inf)
    row_peak = jnp.maximum(jnp.max(cached, axis=-1), own_score)
    cached_w = jnp.exp(cached - row_peak[..., None])
    own_w = jnp.exp(own_score - row_peak)
    row_total = jnp.sum(cached_w, axis=-1) + own_w
    cached_w = cached_w / row_total[..., None]
    own_w = own_w / row_total
    lam_heads = diff_lambda.reshape(1, KV_HEADS, repeat)
    mix_cached = (cached_w[:, :, :, 0] - lam_heads[..., None] * cached_w[:, :, :, 1]).astype(
        jnp.bfloat16
    )
    mix_own = (own_w[..., 0] - lam_heads * own_w[..., 1]).astype(jnp.bfloat16)
    head_raw = jnp.einsum(
        "sgrl,slgv->sgrv", mix_cached, cache_vals, preferred_element_type=jnp.float32
    )
    head_raw = (
        head_raw
        + mix_own.astype(jnp.float32)[..., None] * value_rows.astype(jnp.float32)[:, :, None, :]
    )
    head_out = rms_scale(head_raw, head_gain, HEAD_EPS) * HEAD_SCALE
    return head_out.astype(jnp.bfloat16).reshape(row_count, HEADS * HEAD_V)


def body(
    tokens,
    norm_gain,
    w_query,
    w_key,
    w_value,
    key_cache,
    value_cache,
    lengths,
    diff_lambda,
    head_gain,
    w_out,
    ffn_gain,
    routing,
    route_weight,
    w_gate,
    w_up,
    w_down,
):
    group_tokens = lax.all_gather(tokens, "tp", axis=0, tiled=True)
    normed = rms_scale(group_tokens.astype(jnp.float32), norm_gain, NORM_EPS).astype(jnp.bfloat16)
    blocks = lax.all_to_all(normed, "ep", split_axis=1, concat_axis=0, tiled=True)
    query_term = jnp.dot(blocks, w_query, preferred_element_type=jnp.float32)
    key_term = jnp.dot(blocks, w_key, preferred_element_type=jnp.float32)
    value_term = jnp.dot(blocks, w_value, preferred_element_type=jnp.float32)
    query_sum, key_sum, value_sum = (
        lax.psum_scatter(query_term, "ep", scatter_dimension=0, tiled=True),
        lax.psum_scatter(key_term, "ep", scatter_dimension=0, tiled=True),
        lax.psum_scatter(value_term, "ep", scatter_dimension=0, tiled=True),
    )
    queries = query_sum.astype(jnp.bfloat16)
    keys_made = key_sum.astype(jnp.bfloat16)
    values_made = value_sum.astype(jnp.bfloat16)
    own_query, new_keys, new_values = (
        lax.all_to_all(queries, "tp", split_axis=0, concat_axis=1, tiled=True),
        lax.all_to_all(keys_made, "tp", split_axis=0, concat_axis=1, tiled=True),
        lax.all_to_all(values_made, "tp", split_axis=0, concat_axis=1, tiled=True),
    )
    head_out = attend(
        own_query, new_keys, new_values, key_cache, value_cache, lengths, diff_lambda, head_gain
    )
    head_rows = lax.all_to_all(head_out, "tp", split_axis=1, concat_axis=0, tiled=True)
    partial_out = jnp.dot(
        head_rows,
        lax.all_gather(w_out, "ep", axis=1, tiled=True),
        preferred_element_type=jnp.float32,
    )
    attn_sum = lax.psum_scatter(
        partial_out.astype(jnp.bfloat16), "tp", scatter_dimension=0, tiled=True
    ).astype(jnp.float32)
    residual = tokens.astype(jnp.float32) + attn_sum
    ffn_in = rms_scale(residual, ffn_gain, NORM_EPS).astype(jnp.bfloat16)
    group_in = lax.all_gather(ffn_in, "tp", axis=0, tiled=True)
    experts = lax.axis_size("ep")
    capacity = 8 * SEQ_DEV * lax.axis_size("tp") // experts
    group_rows = group_in.shape[0]
    picks = routing.reshape(-1)
    choose = (picks[:, None] == jnp.arange(experts)[None, :]).astype(jnp.int32)
    earlier = jnp.cumsum(choose, axis=0) - choose
    slot_in = jnp.sum(earlier * choose, axis=1)
    slot_ids = (picks * capacity + slot_in).reshape(group_rows, TOPK)
    slot_hit = slot_ids[:, :, None] == jnp.arange(experts * capacity)[None, None, :]
    dispatch = jnp.sum(slot_hit, axis=1).astype(jnp.bfloat16)
    outgoing = jnp.einsum(
        "rj,rd->jd", dispatch, group_in, preferred_element_type=jnp.float32
    ).astype(jnp.bfloat16)
    outgoing = outgoing.reshape(experts, capacity, group_in.shape[1])
    arrived = lax.all_to_all(outgoing, "ep", split_axis=0, concat_axis=0, tiled=True)
    sources, slot_count, feat_dim = arrived.shape
    flat_rows = arrived.reshape(sources * slot_count, feat_dim)
    gate_pre = jnp.dot(flat_rows, w_gate[0], preferred_element_type=jnp.float32)
    up_pre = jnp.dot(flat_rows, w_up[0], preferred_element_type=jnp.float32)
    hidden = (jax.nn.silu(gate_pre) * up_pre).astype(jnp.bfloat16)
    partial_down = jnp.dot(hidden, w_down[0], preferred_element_type=jnp.float32)
    summed = lax.psum_scatter(
        partial_down.astype(jnp.bfloat16), "tp", scatter_dimension=1, tiled=True
    )
    expert_rows = summed.reshape(sources, slot_count, summed.shape[1])
    returned = lax.all_to_all(expert_rows, "ep", split_axis=0, concat_axis=0, tiled=True)
    combine = jnp.sum(slot_hit.astype(jnp.float32) * route_weight[:, :, None], axis=1)
    flat_back = returned.reshape(experts * capacity, returned.shape[2]).astype(jnp.float32)
    moe_cols = jnp.dot(combine, flat_back, precision=lax.Precision.HIGHEST)
    moe_own = lax.all_to_all(moe_cols, "tp", split_axis=0, concat_axis=1, tiled=True)
    return ((residual + moe_own).astype(jnp.bfloat16), new_keys, new_values)


F32 = jnp.float32
BF16 = jnp.bfloat16
LANES = 128


WO_CUTS = (6, 2)
WO_FIRST = 1


def fused_kernel(
    ep_size,
    tp_size,
    tok_hbm,
    norm_gain_hbm,
    wq_hbm,
    wk_hbm,
    wv_hbm,
    kc_hbm,
    vc_hbm,
    len_s,
    lam_hbm,
    head_gain_hbm,
    wo_hbm,
    ffn_gain_hbm,
    routing_hbm,
    rweight_hbm,
    wg_hbm,
    wu_hbm,
    wd_hbm,
    out_ref,
    nk_ref,
    nv_ref,
    tok_v,
    norm_gain,
    head_gain,
    ffn_gain,
    lam_s,
    routing_s,
    rweight_s,
    wqkv,
    kc,
    kt,
    vc,
    wo,
    wg,
    wu,
    wd,
    a_send,
    a_recv,
    b_send,
    b_recv,
    c_send,
    c_recv,
    r_send,
    r_recv,
    e_send,
    e_recv,
    stage,
    raw_keep,
    gate_acc,
    up_acc,
    load_sems,
    send_sems,
    recv_sems,
    block_sems,
    wo_send_sems,
    wo_recv_sems,
):
    n_dev = ep_size * tp_size
    my_ep = lax.axis_index("ep")
    my_tp = lax.axis_index("tp")
    me = my_ep * tp_size + my_tp
    my_row, my_col = my_tp // 2, lax.rem(my_tp, 2)
    other_col = 1 - my_col
    my_slot = my_ep * 2 + my_row
    slots = 2 * ep_size
    width = tok_v.shape[1]
    feat = width // ep_size
    pieces = feat // LANES
    q_cols = wq_hbm.shape[1]
    q_rows = q_cols // LANES
    repeat = HEADS // KV_HEADS
    tile_rows = width // LANES
    a_rows = a_send.shape[1]
    b_tiles, b_rows = b_send.shape[1:3]
    b_span = b_tiles * b_rows

    def flips(index, size):
        bits = [lax.rem(index // (1 << b), 2) for b in range(size.bit_length() - 1)]
        return [
            sum(
                ((1 - bit) if (mask >> b) & 1 else bit) * (1 << b)
                for b, bit in enumerate(bits)
            )
            for mask in range(size)
        ]

    ep_of = flips(my_ep, ep_size)
    tp_of = flips(my_tp, tp_size)
    everyone = [
        (i, j) for i in reversed(range(ep_size)) for j in reversed(range(tp_size)) if i or j
    ]
    row_to = (my_row, 1 - my_row)
    targets = [
        (i, row_to[flip] * 2 + col)
        for col in range(2)
        for flip in (1, 0)
        for i in reversed(range(1, ep_size))
    ] + [(0, tp_of[j]) for j in reversed(range(1, tp_size))]
    cross = [(i, j) for j in (3, 1) for i in reversed(range(ep_size))]

    barrier = pltpu.get_barrier_semaphore()
    for i, j in everyone:
        pl.semaphore_signal(
            barrier,
            inc=1,
            device_id={"ep": ep_of[i], "tp": tp_of[j]},
            device_id_type=pl.DeviceIdType.MESH,
        )

    wo_rows = wo_hbm.shape[0]
    near_cols = pl.ds(pl.multiple_of(my_row * LANES, LANES), LANES)
    far_cols = pl.ds(pl.multiple_of((1 - my_row) * LANES, LANES), LANES)
    cuts = [wo_rows * eighths // 8 for eighths in WO_CUTS]
    spans = [pl.ds(sum(cuts[:n]), count) for n, count in enumerate(cuts)]
    wo_ships = []

    def wo_push(n):
        wo_ships.append(
            ship(
                wo_hbm.at[spans[n], far_cols],
                wo.at[my_tp, spans[n]],
                0,
                2,
                wo_send_sems.at[n],
                wo_recv_sems.at[n],
            )
        )

    def wo_forward(n):
        at = len(cuts) + 1 + n
        block = wo.at[tp_of[2], spans[n]]
        arrive(block, wo_recv_sems.at[n])
        wo_ships.append(ship(block, block, 0, 1, wo_send_sems.at[at], wo_recv_sems.at[at]))

    load_list = [
        (tok_hbm, tok_v),
        (norm_gain_hbm, norm_gain),
        (wq_hbm, wqkv.at[my_col, :, pl.ds(0, q_cols)]),
        (wk_hbm, wqkv.at[my_col, :, pl.ds(q_cols, LANES)]),
        (wv_hbm, wqkv.at[my_col, :, pl.ds(q_cols + LANES, LANES)]),
        (kc_hbm.at[0], kc),
        (vc_hbm.at[0], vc),
        (lam_hbm, lam_s),
        (head_gain_hbm, head_gain),
        (wo_hbm.at[:, near_cols], wo.at[my_tp]),
        (ffn_gain_hbm, ffn_gain),
        (routing_hbm, routing_s),
        (rweight_hbm, rweight_s),
        (wg_hbm.at[0], wg),
        (wu_hbm.at[0], wu),
        (wd_hbm.at[0], wd),
    ]
    loads = [
        pltpu.make_async_copy(src, dst, load_sems.at[i]) for i, (src, dst) in enumerate(load_list)
    ]
    for load in loads:
        load.start()

    def ship_to(src, dst, i, to, send_sem, recv_sem):
        copy = pltpu.make_async_remote_copy(
            src_ref=src,
            dst_ref=dst,
            send_sem=send_sem,
            recv_sem=recv_sem,
            device_id={"ep": ep_of[i], "tp": to},
            device_id_type=pl.DeviceIdType.MESH,
        )
        copy.start()
        return copy

    def ship(src, dst, i, j, send_sem, recv_sem):
        return ship_to(src, dst, i, tp_of[j], send_sem, recv_sem)

    def arrive(target, sem):
        pltpu.make_async_copy(target, target, sem).wait()

    loads[0].wait()
    loads[1].wait()
    tok = tok_v[...].astype(F32)
    mean_sq = jnp.mean(tok * tok, axis=-1, keepdims=True)
    normed = tok * lax.rsqrt(mean_sq + NORM_EPS) * norm_gain[...]
    for e in range(ep_size):
        for p in range(pieces):
            cols = slice(e * feat + p * LANES, e * feat + (p + 1) * LANES)
            at = e * a_rows + p
            stage[at : at + 1, :] = normed[:, cols]
            stage[at + pieces : at + pieces + 1, :] = tok[:, cols]
    for e in range(ep_size):
        a_send[e] = stage[e * a_rows : (e + 1) * a_rows, :].astype(BF16)
    pl.semaphore_wait(barrier, n_dev - 1)
    for i, j in cross:
        ship(a_send.at[ep_of[i]], a_recv.at[my_slot], i, j, send_sems.at[0], recv_sems.at[0])
    pair_ships = [
        ship(
            src,
            wqkv.at[my_col, :, pl.ds(first, src.shape[1])],
            0,
            1,
            wo_send_sems.at[2 * len(cuts) + 1 + n],
            wo_recv_sems.at[2 * len(cuts) + 1 + n],
        )
        for n, (src, first) in enumerate(
            ((wq_hbm, 0), (wk_hbm, q_cols), (wv_hbm, q_cols + LANES))
        )
    ]
    for n in range(WO_FIRST):
        wo_push(n)
    arrive(a_recv, recv_sems.at[0])
    for n in range(slots):
        stage[n * a_rows : (n + 1) * a_rows, :] = a_recv[n].astype(F32)
    blocks = jnp.concatenate(
        [stage[pl.ds(p, slots, stride=a_rows), :] for p in range(pieces)], axis=1
    ).astype(BF16)
    raw_keep[...] = stage[pl.ds(pieces + my_row, slots, stride=a_rows), :]

    for i in range(2, 5):
        loads[i].wait()
    for n, (first, count) in enumerate(((0, q_cols), (q_cols, LANES), (q_cols + LANES, LANES))):
        arrive(
            wqkv.at[other_col, :, pl.ds(first, count)], wo_recv_sems.at[2 * len(cuts) + 1 + n]
        )
    for col in range(2):
        proj = jnp.dot(blocks, wqkv[col], preferred_element_type=F32)
        rows_at = [col * q_rows + j for j in range(q_rows)] + [2 * q_rows + col, 2 * q_rows + 2 + col]
        for j, at in enumerate(rows_at):
            stage[pl.ds(at, slots, stride=b_span), :] = proj[:, j * LANES : (j + 1) * LANES]
    for n in range(slots):
        for k in range(b_tiles):
            at = n * b_span + k * b_rows
            b_send[n, k] = stage[at : at + b_rows, :].astype(BF16)
    for i, j in cross:
        to = ep_of[i] * 2 + tp_of[j] // 2
        ship(b_send.at[to], b_recv.at[my_slot], i, j, send_sems.at[1], recv_sems.at[1])
    for n in range(WO_FIRST, len(cuts)):
        wo_push(n)
    wo_ships.append(
        ship(
            wo_hbm.at[:, near_cols],
            wo.at[my_tp],
            0,
            1,
            wo_send_sems.at[len(cuts)],
            wo_recv_sems.at[len(cuts)],
        )
    )
    loads[5].wait()
    for part in range(kc.shape[1] // HEAD_QK):
        cols = slice(part * HEAD_QK, (part + 1) * HEAD_QK)
        kt[cols, :] = kc[:, cols].T
    for i in range(6, 9):
        loads[i].wait()
    rows = 2 * repeat
    length = len_s[0]
    positions = kc.shape[0]
    first_map = lax.rem(lax.broadcasted_iota(jnp.int32, (rows, LANES), 0), 2) == 0
    valid = lax.broadcasted_iota(jnp.int32, (rows, positions), 1) < length
    head_at = lax.broadcasted_iota(jnp.int32, (rows, LANES), 0) // 2
    lams = []
    for g in range(KV_HEADS):
        lam = jnp.zeros((rows, LANES), F32)
        for r in range(repeat):
            lam = jnp.where(head_at == r, lam_s[g * repeat + r], lam)
        lams.append(lam)
    arrive(b_recv, recv_sems.at[1])
    for n in range(WO_FIRST):
        wo_forward(n)
    k_parts, v_parts = [], []
    for row in range(2):
        total = b_recv[row].astype(F32)
        for e in range(1, ep_size):
            total = total + b_recv[e * 2 + row].astype(F32)
        for k in range(2 * q_rows // b_rows):
            at = row * 2 * q_rows + k * b_rows
            stage[at : at + b_rows, :] = total[k]
        for col in range(2):
            t = row * 2 + col
            key_row = total[b_tiles - 1, col : col + 1].astype(BF16)
            value_row = total[b_tiles - 1, 2 + col : 3 + col].astype(BF16)
            nk_ref[:, t * LANES : (t + 1) * LANES] = key_row
            nv_ref[:, t * LANES : (t + 1) * LANES] = value_row
            k_parts.append(key_row.astype(F32))
            v_parts.append(value_row.astype(F32))
    q_all = stage[0 : tp_size * q_rows, :].astype(BF16)

    scale = HEAD_QK ** (-0.5)
    scores, owns = [], []
    for g in range(KV_HEADS):
        q32 = q_all[g * rows : (g + 1) * rows].astype(F32)
        base = g * 2 * HEAD_QK
        both = jnp.concatenate(
            [jnp.where(first_map, q32, 0.0), jnp.where(first_map, 0.0, q32)], axis=1
        ).astype(BF16)
        score = jnp.dot(both, kt[base : base + 2 * HEAD_QK, :], preferred_element_type=F32)
        scores.append(jnp.where(valid, score * scale, -jnp.inf))
        owns.append(
            jnp.sum(
                q32 * jnp.where(first_map, k_parts[2 * g], k_parts[2 * g + 1]),
                axis=-1,
                keepdims=True,
            )
            * scale
        )
    mixes, mixes_own = [], []
    for score, own, lam in zip(scores, owns, lams):
        peak = jnp.maximum(jnp.max(score, axis=-1, keepdims=True), own)
        weight = jnp.exp(score - peak)
        own_weight = jnp.exp(own - peak)
        norm = jnp.sum(weight, axis=-1, keepdims=True) + own_weight
        weight = weight / norm
        own_weight = jnp.broadcast_to(own_weight / norm, (rows, LANES))
        mixes.append((weight - lam[:, 0:1] * pltpu.roll(weight, rows - 1, 0)).astype(BF16))
        mixes_own.append(
            (own_weight - lam * pltpu.roll(own_weight, rows - 1, 0)).astype(BF16).astype(F32)
        )
    raws = [
        jnp.dot(mix, vc[:, g * HEAD_V : (g + 1) * HEAD_V], preferred_element_type=F32)
        for g, mix in enumerate(mixes)
    ]
    for g, (raw, mix_own) in enumerate(zip(raws, mixes_own)):
        raw = raw + jnp.concatenate(
            [mix_own * v_parts[2 * g], mix_own * v_parts[2 * g + 1]], axis=1
        )
        mean_sq = jnp.mean(raw * raw, axis=-1, keepdims=True)
        head = raw * lax.rsqrt(mean_sq + HEAD_EPS) * head_gain[...] * HEAD_SCALE
        c_send[g * rows : (g + 1) * rows, :] = jnp.where(
            first_map, head[:, 0:LANES], pltpu.roll(head[:, LANES : 2 * LANES], 1, 0)
        ).astype(BF16)
    for i, j in cross:
        ship(c_send, c_recv.at[my_slot], i, j, send_sems.at[2], recv_sems.at[2])
    for n in range(WO_FIRST, len(cuts)):
        wo_forward(n)
    loads[9].wait()
    loads[10].wait()
    arrive(wo.at[tp_of[1]], wo_recv_sems.at[len(cuts)])
    for n in range(len(cuts)):
        arrive(wo.at[tp_of[3], spans[n]], wo_recv_sems.at[len(cuts) + 1 + n])
    arrive(c_recv, recv_sems.at[2])

    head_rows = c_send.shape[0]
    tiles_block = head_rows // tp_size
    for n in range(slots):
        part = c_recv[n].astype(F32)
        for t in range(tp_size):
            at = (t * slots + n) * tiles_block
            stage[at : at + tiles_block, :] = part[t * tiles_block : (t + 1) * tiles_block]

    total = raw_keep[...]
    for t in range(tp_size):
        lhs = jnp.concatenate(
            [
                stage[pl.ds(t * tiles_block * slots + r, slots, stride=tiles_block), :]
                for r in range(tiles_block)
            ],
            axis=1,
        ).astype(BF16)
        total = total + jnp.dot(lhs, wo[t], preferred_element_type=F32)
    r_send[...] = total.astype(BF16)
    for i, to in targets:
        ship_to(r_send, r_recv.at[my_ep, my_tp], i, to, send_sems.at[3], block_sems.at[i])
    r_recv[my_ep, my_tp] = r_send[...]

    loads[13].wait()
    loads[14].wait()
    low, high = lax.rem(my_ep // 2, 2), my_ep // 4
    inner = low + high - 2 * low * high
    order = [(at_end, inside) for at_end, inside in zip((1, 0, 5, 4, 3, 2, 7, 6), (1, 0, 7, 6, 3, 2, 5, 4))]

    def pick(at_end, inside):
        return inside * inner + at_end * (1 - inner)

    square = jnp.zeros((n_dev, LANES), F32)
    for step, (at_end, inside) in enumerate(order):
        place = pick(ep_of[at_end], ep_of[inside])
        count = tp_size if at_end else tp_size - 1
        arrive(r_recv.at[place, pl.ds(0, count)], block_sems.at[pick(at_end, inside)])
        at = pl.multiple_of(place * feat, feat)
        parts = []
        for p in range(pieces):
            part = r_recv[place, 2 * p : 2 * p + 2].astype(F32).reshape(n_dev, LANES)
            square = square + part * part
            parts.append(part * ffn_gain[:, pl.ds(at + p * LANES, LANES)])
        scaled = jnp.concatenate(parts, axis=1).astype(BF16)
        gate_add = jnp.dot(scaled, wg[pl.ds(at, feat), :], preferred_element_type=F32)
        up_add = jnp.dot(scaled, wu[pl.ds(at, feat), :], preferred_element_type=F32)
        if step == 0:
            gate_acc[...] = gate_add
            up_acc[...] = up_add
        elif step < ep_size - 1:
            gate_acc[...] += gate_add
            up_acc[...] += up_add
    row_scale = lax.rsqrt(jnp.sum(square, axis=-1, keepdims=True) * (1.0 / width) + NORM_EPS)
    gate = (gate_acc[...] + gate_add) * row_scale
    up = (up_acc[...] + up_add) * row_scale
    hidden = (gate / (1.0 + jnp.exp(-gate)) * up).astype(BF16)
    loads[15].wait()

    def row_of(e, t):
        return (1 - lax.rem(t, 2)) * slots + e * 2 + t // 2

    down = jnp.dot(hidden, wd[...], preferred_element_type=F32)
    for j in range(tile_rows):
        stage[pl.ds(j, n_dev, stride=tile_rows), :] = down[:, j * LANES : (j + 1) * LANES]
    e_send[...] = stage[...].astype(BF16).reshape(n_dev, tile_rows, LANES)
    for i, to in targets:
        ship_to(
            e_send.at[row_of(ep_of[i], to)], e_recv.at[me], i, to, send_sems.at[4], recv_sems.at[3]
        )
    e_recv[me] = e_send[row_of(my_ep, my_tp)]
    loads[11].wait()
    loads[12].wait()
    for e in range(ep_size):
        for p in range(pieces):
            at = (e * pieces + p) * slots
            stage[at : at + slots, :] = r_recv[e, 2 * p + other_col].astype(F32)
    result = stage[pl.ds(my_slot, tile_rows, stride=slots), :]
    shares = []
    for e in range(ep_size):
        share = jnp.float32(0.0)
        for k in range(TOPK):
            share = share + jnp.where(routing_s[k, my_tp] == e, rweight_s[k, my_tp], 0.0)
        shares.append(share)
    for ship_done in wo_ships + pair_ships:
        ship_done.wait_send()
    for phase, part in (
        (0, a_recv),
        (1, b_recv),
        (2, c_recv),
    ):
        arrive(part, send_sems.at[phase])
    arrive(e_recv.at[pl.ds(0, n_dev - 1)], send_sems.at[3])
    arrive(e_recv.at[pl.ds(0, n_dev - 1)], recv_sems.at[3])
    for e in range(ep_size):
        total = e_recv[e * tp_size].astype(F32)
        for t in range(1, tp_size):
            total = total + e_recv[e * tp_size + t].astype(F32)
        result = result + total.astype(BF16).astype(F32) * shares[e]
    for j in range(tile_rows):
        out_ref[:, j * LANES : (j + 1) * LANES] = result[j : j + 1].astype(BF16)
    arrive(e_recv.at[pl.ds(0, n_dev - 1)], send_sems.at[4])


def write_kernel(result_ref, keys_ref, values_ref, result_out, keys_out, values_out, sems):
    copies = [
        pltpu.make_async_copy(src, dst, sems.at[i])
        for i, (src, dst) in enumerate(
            ((result_ref, result_out), (keys_ref, keys_out), (values_ref, values_out))
        )
    ]
    for copy in copies:
        copy.start()
    for copy in copies:
        copy.wait()


def fused_body(
    tokens,
    norm_gain,
    w_query,
    w_key,
    w_value,
    key_cache,
    value_cache,
    lengths,
    diff_lambda,
    head_gain,
    w_out,
    ffn_gain,
    routing,
    route_weight,
    w_gate,
    w_up,
    w_down,
):
    ep_size, tp_size = lax.axis_size("ep"), lax.axis_size("tp")
    n_dev = ep_size * tp_size
    width = tokens.shape[1]
    feat = width // ep_size
    vmem = pl.BlockSpec(memory_space=pltpu.VMEM)
    hbm = pl.BlockSpec(memory_space=pltpu.HBM)
    tile_rows = width // LANES
    proj_cols = w_query.shape[1] + w_key.shape[1] + w_value.shape[1]
    head_tiles = HEADS * HEAD_V // LANES
    scratch = [
        pltpu.VMEM(tokens.shape, BF16),
        pltpu.VMEM((1, width), F32),
        pltpu.VMEM((1, HEAD_V), F32),
        pltpu.VMEM((1, width), F32),
        pltpu.SMEM(diff_lambda.shape, F32),
        pltpu.SMEM(routing.shape[::-1], jnp.int32),
        pltpu.SMEM(route_weight.shape[::-1], F32),
        pltpu.VMEM((2, feat, proj_cols), BF16),
        pltpu.VMEM(key_cache.shape[1:], BF16),
        pltpu.VMEM(key_cache.shape[:0:-1], BF16),
        pltpu.VMEM(value_cache.shape[1:], BF16),
        pltpu.VMEM((tp_size, w_out.shape[0], LANES), BF16),
        pltpu.VMEM(w_gate.shape[1:], BF16),
        pltpu.VMEM(w_up.shape[1:], BF16),
        pltpu.VMEM(w_down.shape[1:], BF16),
        pltpu.VMEM((ep_size, 4, LANES), BF16),
        pltpu.VMEM((2 * ep_size, 4, LANES), BF16),
        pltpu.VMEM((2 * ep_size, 5, 4, LANES), BF16),
        pltpu.VMEM((2 * ep_size, 5, 4, LANES), BF16),
        pltpu.VMEM((head_tiles, LANES), BF16),
        pltpu.VMEM((2 * ep_size, head_tiles, LANES), BF16),
        pltpu.VMEM((2 * ep_size, LANES), BF16),
        pltpu.VMEM((ep_size, tp_size, 2 * ep_size, LANES), BF16),
        pltpu.VMEM((n_dev, tile_rows, LANES), BF16),
        pltpu.VMEM((n_dev, tile_rows, LANES), BF16),
        pltpu.VMEM((n_dev * 16, LANES), F32),
        pltpu.VMEM((2 * ep_size, LANES), F32),
        pltpu.VMEM((n_dev, w_gate.shape[2]), F32),
        pltpu.VMEM((n_dev, w_gate.shape[2]), F32),
        pltpu.SemaphoreType.DMA((16,)),
        pltpu.SemaphoreType.DMA((5,)),
        pltpu.SemaphoreType.DMA((4,)),
        pltpu.SemaphoreType.DMA((ep_size,)),
        pltpu.SemaphoreType.DMA((2 * len(WO_CUTS) + 4,)),
        pltpu.SemaphoreType.DMA((2 * len(WO_CUTS) + 4,)),
    ]
    call = pl.pallas_call(
        functools.partial(fused_kernel, ep_size, tp_size),
        name="fused_layer",
        out_shape=(
            jax.ShapeDtypeStruct(tokens.shape, BF16),
            jax.ShapeDtypeStruct((1, key_cache.shape[2]), BF16),
            jax.ShapeDtypeStruct((1, value_cache.shape[2]), BF16),
        ),
        in_specs=[hbm] * 7 + [pl.BlockSpec(memory_space=pltpu.SMEM)] + [hbm] * 9,
        out_specs=(vmem, vmem, vmem),
        scratch_shapes=scratch,
        compiler_params=pltpu.CompilerParams(
            collective_id=0, has_side_effects=True, vmem_limit_bytes=28 * 1024 * 1024
        ),
    )
    operands = (
        tokens,
        norm_gain.reshape(1, -1),
        w_query,
        w_key,
        w_value,
        key_cache,
        value_cache,
        lengths,
        diff_lambda,
        head_gain.reshape(1, -1),
        w_out,
        ffn_gain.reshape(1, -1),
        routing.T,
        route_weight.T,
        w_gate,
        w_up,
        w_down,
    )
    pinned = [
        array if array is lengths else pltpu.with_memory_space_constraint(array, pltpu.HBM)
        for array in operands
    ]
    made = call(*pinned)
    return pl.pallas_call(
        write_kernel,
        name="write_out",
        out_shape=tuple(jax.ShapeDtypeStruct(array.shape, array.dtype) for array in made),
        in_specs=[vmem] * len(made),
        out_specs=tuple(pl.BlockSpec(memory_space=pl.ANY) for _ in made),
        scratch_shapes=[pltpu.SemaphoreType.DMA((len(made),))],
        compiler_params=pltpu.CompilerParams(vmem_limit_bytes=1024 * 1024),
    )(*made)


def layer(*arrays):
    tokens, w_query, w_key = arrays[0], arrays[2], arrays[3]
    feat = tokens.shape[1] // lax.axis_size("ep")
    whole_tiles = (
        tokens.shape[0] == 1
        and w_key.shape[1] == LANES
        and w_query.shape[1] == 8 * LANES
        and feat == 2 * LANES
        and tokens.shape[1] == 16 * LANES
    )
    return fused_body(*arrays) if whole_tiles else body(*arrays)


def solution(mesh):
    placed = (
        P(("ep", "tp"), None),
        P(),
        P("ep", "tp"),
        P("ep", "tp"),
        P("ep", "tp"),
        P(("ep", "tp"), None, None),
        P(("ep", "tp"), None, None),
        P(("ep", "tp")),
        P(),
        P(),
        P("tp", "ep"),
        P(),
        P("ep", None),
        P("ep", None),
        P("ep", None, "tp"),
        P("ep", None, "tp"),
        P("ep", "tp", None),
    )
    return jax.shard_map(
        layer,
        mesh=mesh,
        in_specs=placed,
        out_specs=(P(("ep", "tp"), None), P(("ep", "tp"), None), P(("ep", "tp"), None)),
        check_vma=False,
    )
```
